512 devices in a mesh: sp: 128 (over z, x, core), tp: 4 (over y).
Axes of the slice: x: 4, y: 4, z: 16, core: 2. Of those that a mesh axis runs over, the one named last changes fastest.
Arguments:
- query_main: bfloat16 [16384, 2048], P('sp', 'tp'), may hold values from -6 to 6
- query_rotary: bfloat16 [16384, 1024], P('sp', 'tp'), may hold values from -7 to 7
- latent: bfloat16 [16384, 512], P('sp'), may hold values from -24 to 24
- key_rotary: bfloat16 [16384, 64], P('sp'), may hold values from -8 to 8
- key_weight: bfloat16 [512, 2048], P(None, 'tp'), may hold values from -0.25 to 0.25
- value_weight: bfloat16 [512, 2048], P(None, 'tp'), may hold values from -0.25 to 0.25
- head_output: bfloat16 [16384, 2048], P('sp', 'tp'), may hold values from -2 to 2
- output_grad: bfloat16 [16384, 2048], P('sp', 'tp'), may hold values from -128 to 128
- row_logsum: float32 [16, 16384], P('tp', 'sp'), may hold values from 3 to 16, as said below
Outputs:
- grad_query_main: float32 [16384, 2048], P('sp', 'tp')
- grad_query_rotary: float32 [16384, 1024], P('sp', 'tp')
- grad_latent: float32 [16384, 512], P('sp')
- grad_key_rotary: float32 [16384, 64], P('sp')
- grad_key_weight: float32 [512, 2048], P('sp', 'tp')
The draws below stay inside these ranges and needn't reach their ends.
Inputs may be any that keep to these rules, and one draw needn't show every extreme that they name: With p the place of token i in its sequence and q = i % 128, row_logsum[h, i] minus the logarithm of (p + 1 + 54 (q + 1)) lies between -0.3 and 1.5.
All inputs are finite; a program needn't handle non-finite values.
Results may differ from the reference program's by a relative error of at most 0.003.
The reference program's roundings to bfloat16 on the way (of `query_latent`, `grad_rows`, `weights_low`, `dscores_low` and `mixed_low`) count: a program that leaves them out, or rounds other values in their place, can miss the bound.
Values may be sent and summed in bfloat16 or wider, within the bound.
No kernel may reach another device: no remote copies, remote signals or barrier semaphores. Data moves between devices by JAX's collectives and lax.ppermute only.
A program may use at most 64 MiB of HBM per device.

```python
import math
import jax
import jax.numpy as jnp
from jax import lax

TOK_DEV = 128
HEADS = 16
KDIM = 128
RDIM = 64
VDIM = 128
LATENT = 512
SPAN = 32
LEAD = 8
SEQS = 5
TOKENS = 16384
N_SP = 128


own_mass = 54.0


def block_signs(key):
    picks = jax.random.randint(jax.random.fold_in(key, 7), (TOKENS // TOK_DEV, RDIM), 0, 2)
    table = picks.astype(jnp.float32) * 2.0 - 1.0
    return table[jnp.arange(TOKENS) // TOK_DEV]


def noise_field(key, shape):
    return jnp.clip(jax.random.normal(key, shape, jnp.float32), -6.0, 6.0)


def draw_query_rotary(key, part):
    signs = block_signs(key)
    noise = noise_field(jax.random.fold_in(key, 11), (TOKENS, HEADS, RDIM))
    return (noise + signs[:, None, :]).reshape(TOKENS, HEADS * RDIM).astype(jnp.bfloat16)


def draw_key_rotary(key, part):
    signs = block_signs(key)
    noise = noise_field(jax.random.fold_in(key, 13), (TOKENS, RDIM))
    strength = 4.0 * (KDIM + RDIM) ** 0.5 / RDIM
    return (noise + strength * signs).astype(jnp.bfloat16)


def draw_row_logsum(key, part):
    token = jnp.arange(TOKENS)
    device = token // TOK_DEV
    sequence = (device + LEAD) // SPAN
    first_device = jnp.maximum(sequence * SPAN - LEAD, 0)
    place = (token - first_device * TOK_DEV + 1).astype(jnp.float32)
    inside = (token % TOK_DEV + 1).astype(jnp.float32)
    total = place + own_mass * inside
    offset = jax.random.uniform(key, (HEADS, TOKENS), jnp.float32, 0.2, 1.2)
    return jnp.log(total)[None, :] + offset


def with_spikes(drawn, own_key, source, target, parts, factor):
    def block_of(axis_at):
        return (jnp.arange(drawn.shape[axis_at]) // (drawn.shape[axis_at] // parts)).reshape((-1,) + (1,) * (drawn.ndim - 1 - axis_at))

    near = jax.random.permutation(own_key, parts)[block_of(target)]
    second = (block_of(target) + parts // 2) % parts
    return jnp.where((block_of(source) == near) | (block_of(source) == second), factor * drawn, drawn)


def levels(key, shape, split, smallest, top_value):
    gain = 1.0
    for axis_at, parts in split:
        heights = jax.random.uniform(jax.random.fold_in(jax.random.fold_in(key, 6), axis_at), (parts,), jnp.float32, smallest / len(split), top_value / len(split))
        gain = gain * jnp.repeat(jnp.exp(heights), shape[axis_at] // parts).reshape((-1,) + (1,) * (len(shape) - 1 - axis_at))
    return gain


def centred(stream_key, extent, scale, bound, pieces=(), held_as=jnp.bfloat16):
    entries = jax.random.normal(stream_key, extent, jnp.float32) * scale
    if len(pieces) > 0:
        entries = levels(stream_key, extent, pieces, -0.22, 0.18) * entries
    return jnp.clip(entries, min=-bound, max=bound).astype(held_as)


def noise_with(own_key, shape, spread, most, split, heavy, held_as=jnp.bfloat16):
    entries = spread * jax.random.normal(own_key, shape, jnp.float32)
    if split:
        entries = entries * levels(own_key, shape, split, -0.22, 0.18)
    return jnp.clip(with_spikes(entries, jax.random.fold_in(own_key, 3), *heavy), -most, most).astype(held_as)


def setup_inputs(seed: int = 0) -> dict:
    seeds = jax.random.split(jax.random.key(seed), 10)
    query_main = centred(seeds[0], (TOKENS, HEADS * KDIM), 1.0, 6.0, ((0, 128), (1, 4)))
    query_rotary = draw_query_rotary(jax.random.fold_in(seeds[9], 71), 0)
    latent = noise_with(seeds[2], (TOKENS, LATENT), 1.0, 24.0, ((0, 128),), (0, 1, 128, 5.5))
    key_rotary = draw_key_rotary(jax.random.fold_in(seeds[9], 71), 0)
    key_weight = centred(seeds[4], (LATENT, HEADS * KDIM), LATENT ** -0.5, 0.25, ((1, 4),))
    value_weight = centred(seeds[5], (LATENT, HEADS * VDIM), LATENT ** -0.5, 0.25, ((1, 4),))
    head_output = centred(seeds[6], (TOKENS, HEADS * VDIM), 0.3, 2.0, ((0, 128), (1, 4)))
    output_grad = noise_with(seeds[7], (TOKENS, HEADS * VDIM), 6.0, 128.0, ((0, 128), (1, 4)), (0, 1, 128, 5.5))
    row_logsum = draw_row_logsum(jax.random.fold_in(seeds[9], 71), 0)
    return {"query_main": query_main, "query_rotary": query_rotary, "latent": latent, "key_rotary": key_rotary, "key_weight": key_weight, "value_weight": value_weight, "head_output": head_output, "output_grad": output_grad, "row_logsum": row_logsum}


def sequence_grads(lat_seq, rot_seq, query_latent, grad_rows, rot_query, row_logs, row_terms, factor, width):
    wide = jnp.float32
    blocks = lat_seq.shape[0] // width
    heads = query_latent.shape[1]
    lat_all = lat_seq.astype(wide)
    rot_all = rot_seq.astype(wide)
    qlat_all = query_latent.astype(wide)
    grows_all = grad_rows.astype(wide)
    qrot_all = rot_query.astype(wide)

    def query_block(carry, query_index):
        acc_lat, acc_rot = carry
        query_start = (query_index * width).astype(jnp.int32)
        qlat = lax.dynamic_slice_in_dim(qlat_all, query_start, width, 0)
        grows = lax.dynamic_slice_in_dim(grows_all, query_start, width, 0)
        qrot = lax.dynamic_slice_in_dim(qrot_all, query_start, width, 0)
        logs = lax.dynamic_slice_in_dim(row_logs, query_start, width, 0)
        terms = lax.dynamic_slice_in_dim(row_terms, query_start, width, 0)
        query_place = query_start + jnp.arange(width, dtype=jnp.int32)

        def key_block(key_index, inner):
            def visit(state):
                mixed_sum, rot_sum, acc_lat, acc_rot = state
                key_start = (key_index * width).astype(jnp.int32)
                lat_block = lax.dynamic_slice_in_dim(lat_all, key_start, width, 0)
                rot_block = lax.dynamic_slice_in_dim(rot_all, key_start, width, 0)
                key_place = key_start + jnp.arange(width, dtype=jnp.int32)
                seen = key_place[None, :] <= query_place[:, None]
                scores = jnp.einsum("thl,kl->thk", qlat, lat_block) + jnp.einsum("thr,kr->thk", qrot, rot_block)
                weights = jnp.where(seen[:, None, :], jnp.exp(factor * scores - logs[:, :, None]), 0.0)
                slopes = jnp.einsum("thl,kl->thk", grows, lat_block)
                dscores = weights * (slopes - terms[:, :, None])
                weights_low = lax.optimization_barrier(weights.astype(jnp.bfloat16)).astype(wide)
                dscores_low = lax.optimization_barrier(dscores.astype(jnp.bfloat16)).astype(wide)
                mixed_sum = mixed_sum + jnp.einsum("thk,kl->thl", dscores_low, lat_block)
                rot_sum = rot_sum + jnp.einsum("thk,kr->thr", dscores_low, rot_block)
                part_lat = factor * jnp.einsum("thk,thl->kl", dscores_low, qlat) + jnp.einsum("thk,thl->kl", weights_low, grows)
                part_rot = factor * jnp.einsum("thk,thr->kr", dscores_low, qrot)
                old_lat = lax.dynamic_slice_in_dim(acc_lat, key_start, width, 0)
                old_rot = lax.dynamic_slice_in_dim(acc_rot, key_start, width, 0)
                acc_lat = lax.dynamic_update_slice_in_dim(acc_lat, old_lat + part_lat, key_start, 0)
                acc_rot = lax.dynamic_update_slice_in_dim(acc_rot, old_rot + part_rot, key_start, 0)
                return mixed_sum, rot_sum, acc_lat, acc_rot

            def keep(state):
                return state

            return lax.cond(key_index <= query_index, visit, keep, inner)

        start_state = (jnp.zeros((width, heads, lat_all.shape[1]), wide), jnp.zeros((width, heads, rot_all.shape[1]), wide), acc_lat, acc_rot)
        mixed_sum, rot_sum, acc_lat, acc_rot = lax.fori_loop(0, blocks, key_block, start_state)
        return (acc_lat, acc_rot), (mixed_sum, rot_sum)

    start = (jnp.zeros(lat_seq.shape, wide), jnp.zeros(rot_seq.shape, wide))
    (acc_lat, acc_rot), (mixed_parts, rot_parts) = lax.scan(query_block, start, jnp.arange(blocks, dtype=jnp.int32))
    mixed = mixed_parts.reshape(lat_seq.shape[0], heads, lat_seq.shape[1])
    rot_sum = rot_parts.reshape(lat_seq.shape[0], heads, rot_seq.shape[1])
    return mixed, rot_sum, acc_lat, acc_rot


def reference(query_main, query_rotary, latent, key_rotary, key_weight, value_weight, head_output, output_grad, row_logsum):
    wide = jnp.float32
    factor = (KDIM + RDIM) ** -0.5
    count = latent.shape[0]
    width = math.gcd(LEAD * TOK_DEV, 512)
    main_query = query_main.reshape(count, HEADS, KDIM).astype(wide)
    rot_query = query_rotary.reshape(count, HEADS, RDIM)
    key_proj = key_weight.reshape(LATENT, HEADS, KDIM).astype(wide)
    value_proj = value_weight.reshape(LATENT, HEADS, VDIM).astype(wide)
    grad_heads = output_grad.reshape(count, HEADS, VDIM).astype(wide)
    query_latent = jnp.einsum("thd,lhd->thl", main_query, key_proj).astype(jnp.bfloat16)
    grad_rows = jnp.einsum("thd,lhd->thl", grad_heads, value_proj).astype(jnp.bfloat16)
    row_terms = jnp.sum(head_output.reshape(count, HEADS, VDIM).astype(wide) * grad_heads, axis=2)
    row_logs = row_logsum.T.astype(wide)
    mixed_list, rot_list, lat_list, key_rot_list = [], [], [], []
    for sequence in range(SEQS):
        first = max(sequence * SPAN - LEAD, 0) * TOK_DEV
        last = min((sequence + 1) * SPAN - LEAD, N_SP) * TOK_DEV
        mixed, rot_sum, acc_lat, acc_rot = sequence_grads(
            latent[first:last], key_rotary[first:last], query_latent[first:last], grad_rows[first:last],
            rot_query[first:last], row_logs[first:last], row_terms[first:last], factor, width)
        mixed_list.append(mixed)
        rot_list.append(rot_sum)
        lat_list.append(acc_lat)
        key_rot_list.append(acc_rot)
    mixed = jnp.concatenate(mixed_list, axis=0)
    rot_sum = jnp.concatenate(rot_list, axis=0)
    grad_latent = jnp.concatenate(lat_list, axis=0)
    grad_key_rotary = jnp.concatenate(key_rot_list, axis=0)
    mixed_low = lax.optimization_barrier(mixed.astype(jnp.bfloat16)).astype(wide)
    grad_query_main = (factor * jnp.einsum("thl,lhd->thd", mixed_low, key_proj)).reshape(count, HEADS * KDIM)
    grad_query_rotary = (factor * rot_sum).reshape(count, HEADS * RDIM)
    grad_key_weight = (factor * jnp.einsum("thl,thd->lhd", mixed_low, main_query)).reshape(LATENT, HEADS * KDIM)
    return (grad_query_main, grad_query_rotary, grad_latent, grad_key_rotary, grad_key_weight)
```

```python
import jax
import jax.numpy as jnp
from jax import lax
from jax.experimental import pallas as pl
from jax.experimental.pallas import tpu as pltpu
from jax.sharding import Mesh
from jax.sharding import PartitionSpec as P

Z, X, C, Y = "sp_0", "sp_1", "sp_2", "tp"
SP = (Z, X, C)
GROUP = 4
bf16 = jnp.bfloat16
f32 = jnp.float32


def shift(block, axis, by):
    peers = lax.axis_size(axis)
    return lax.ppermute(block, axis, [(i, (i + by) % peers) for i in range(peers)])


def exchange(tiles, axis, groups=None):
    return lax.all_to_all(tiles, axis, 0, 0, tiled=True, axis_index_groups=groups)


def dot(a, b, dims):
    return lax.dot_general(a, b, (dims, ((), ())), preferred_element_type=f32)


def pack_kernel(qm, qr, og, ho, logs, lat, rot, qpack, kpack):
    heads, toks = logs.shape
    width = qm.shape[1] // heads
    qpack[:, 0:512] = qm[...]
    qpack[:, 512:768] = qr[...]
    qpack[:, 768:1280] = og[...]
    lane = lax.broadcasted_iota(jnp.int32, (toks, 128), 1)
    extra = jnp.zeros((toks, 128), f32)
    logs_t = logs[...].T
    for h in range(heads):
        cols = slice(h * width, (h + 1) * width)
        term = jnp.sum(ho[:, cols].astype(f32) * og[:, cols].astype(f32), axis=1, keepdims=True)
        for k, value in enumerate((logs_t[:, h : h + 1], term)):
            for part in range(3):
                piece = value.astype(bf16).astype(f32)
                value = value - piece
                extra = jnp.where(lane == (h * 2 + k) * 3 + part, piece, extra)
    qpack[:, 1280:1408] = extra.astype(bf16)
    kpack[:, 0:512] = lat[...]
    kpack[:, 512:576] = rot[...]
    kpack[:, 576:640] = jnp.zeros((toks, 64), bf16)


def pack(qm, qr, og, ho, logs, lat, rot):
    toks = qm.shape[0]
    return pl.pallas_call(
        pack_kernel,
        out_shape=(
            jax.ShapeDtypeStruct((toks, 1408), bf16),
            jax.ShapeDtypeStruct((toks, 640), bf16),
        ),
        name="pack",
    )(qm, qr, og, ho, logs, lat, rot)


def attend_kernel(
    info, q0, q1, q2, q3, k0, k1, k2, k3, kother, wk, wv,
    d0, d1, d2, d3, own, other, wout,
    qcur, kcur, q_s, qt_s, g_s, gt_s, log_s, term_s, acc, ds_acc, w_acc, wt_acc,
):
    heads, toks, width = 4, 128, 128
    factor = 192.0**-0.5
    my_x = info[3]
    my_c = info[4]
    ds_acc[...] = jnp.zeros_like(ds_acc)
    w_acc[...] = jnp.zeros_like(w_acc)
    wt_acc[...] = jnp.zeros_like(wt_acc)
    q_s[:, 576:640] = jnp.zeros((heads * toks, 64), bf16)

    def chunk(g, _):
        for i, ref in enumerate((q0, q1, q2, q3)):

            @pl.when(g == i)
            def _(ref=ref):
                qcur[...] = ref[...]

        extra = qcur[:, 1280:1408].astype(f32)
        for h in range(heads):
            rows = slice(h * toks, (h + 1) * toks)
            cols = slice(h * width, (h + 1) * width)
            qm_h = qcur[:, cols]
            og_h = qcur[:, 768 + h * width : 768 + (h + 1) * width]
            qr_h = qcur[:, 512 + h * 64 : 512 + (h + 1) * 64]
            q_s[rows, 0:512] = dot(qm_h, wk[:, cols], ((1,), (1,))).astype(bf16)
            qt_s[0:512, rows] = dot(wk[:, cols], qm_h, ((1,), (1,))).astype(bf16)
            g_s[rows, :] = dot(og_h, wv[:, cols], ((1,), (1,))).astype(bf16)
            gt_s[:, rows] = dot(wv[:, cols], og_h, ((1,), (1,))).astype(bf16)
            q_s[rows, 512:576] = qr_h
            qt_s[512:576, rows] = qr_h.T
            for k, ref in enumerate((log_s, term_s)):
                at = (h * 2 + k) * 3
                value = extra[:, at : at + 1] + extra[:, at + 1 : at + 2] + extra[:, at + 2 : at + 3]
                ref[rows, :] = jnp.broadcast_to(value, (toks, 128))
        acc[...] = jnp.zeros_like(acc)
        from_x = (my_x - g + GROUP) % GROUP

        def plane(p, _):
            useful = jnp.where(p == 0, from_x >= my_x, info[jnp.maximum(p - 1, 0)] == 1)

            @pl.when(useful)
            def _():
                for i, ref in enumerate((k0, k1, k2, k3)):

                    @pl.when(p == i)
                    def _(ref=ref):
                        kcur[0:toks, :] = ref[...]

                kcur[toks : 2 * toks, :] = kother[p]
                scores = dot(q_s[...], kcur[...], ((1,), (1,)))
                slopes = dot(g_s[...], kcur[:, 0:512], ((1,), (1,)))
                logs = jnp.concatenate([log_s[...]] * 2, axis=1)
                terms = jnp.concatenate([term_s[...]] * 2, axis=1)
                shape = scores.shape
                row = lax.broadcasted_iota(jnp.int32, shape, 0) % toks
                col = lax.broadcasted_iota(jnp.int32, shape, 1)
                key_c = jnp.where(col < toks, my_c, 1 - my_c)
                key_place = (my_x * 2 + key_c) * toks + col % toks
                query_place = (from_x * 2 + my_c) * toks + row
                query_place = query_place + jnp.where(p == 0, 0, 1 << 20)
                weights = jnp.where(key_place <= query_place, jnp.exp(factor * scores - logs), 0.0)
                dscores = (weights * (slopes - terms)).astype(bf16)
                acc[...] += dot(dscores, kcur[...], ((1,), (0,)))
                ds_acc[p] += dot(qt_s[...], dscores, ((1,), (0,)))
                w_acc[p] += dot(gt_s[...], weights.astype(bf16), ((1,), (0,)))

            return 0

        lax.fori_loop(0, GROUP, plane, 0)
        mains, rots = [], []
        for h in range(heads):
            rows = slice(h * toks, (h + 1) * toks)
            cols = slice(h * width, (h + 1) * width)
            mixed = acc[rows, 0:512]
            high = mixed.astype(bf16)
            low = (mixed - high.astype(f32)).astype(bf16)
            w_h = wk[:, cols]
            mains.append(factor * (dot(high, w_h, ((1,), (0,))) + dot(low, w_h, ((1,), (0,)))))
            rots.append(factor * acc[rows, 512:576])
            qm_h = qcur[:, cols]
            wt_acc[cols, :] += dot(qm_h, high, ((0,), (0,))) + dot(qm_h, low, ((0,), (0,)))
        for i, ref in enumerate((d0, d1, d2, d3)):

            @pl.when(g == i)
            def _(ref=ref):
                ref[:, 0:512] = jnp.concatenate(mains, axis=1)
                ref[:, 512:768] = jnp.concatenate(rots, axis=1)

        return 0

    lax.fori_loop(0, GROUP, chunk, 0)
    for p in range(GROUP):
        lat_t = factor * ds_acc[p, 0:512, :] + w_acc[p]
        rot_t = factor * ds_acc[p, 512:576, :]
        both = jnp.concatenate([lat_t, rot_t], axis=0)
        for y in range(4):
            own[y, p] = both[y * 144 : (y + 1) * 144, 0:toks]
            other[y, p] = both[y * 144 : (y + 1) * 144, toks : 2 * toks]
    wout[...] = factor * wt_acc[...].T


def attend(info, qs, ks, kother, wk, wv):
    toks = 128
    out = jax.ShapeDtypeStruct
    vmem = pl.BlockSpec(memory_space=pltpu.VMEM)
    return pl.pallas_call(
        attend_kernel,
        in_specs=[pl.BlockSpec(memory_space=pltpu.SMEM)] + [vmem] * 11,
        out_specs=[vmem] * 7,
        out_shape=[out((toks, 768), f32)] * 4
        + [out((4, GROUP, 144, toks), f32)] * 2
        + [out((512, 512), f32)],
        scratch_shapes=[
            pltpu.VMEM((toks, 1408), bf16),
            pltpu.VMEM((2 * toks, 640), bf16),
            pltpu.VMEM((512, 640), bf16),
            pltpu.VMEM((576, 512), bf16),
            pltpu.VMEM((512, 512), bf16),
            pltpu.VMEM((512, 512), bf16),
            pltpu.VMEM((512, 128), f32),
            pltpu.VMEM((512, 128), f32),
            pltpu.VMEM((512, 640), f32),
            pltpu.VMEM((GROUP, 576, 2 * toks), f32),
            pltpu.VMEM((GROUP, 512, 2 * toks), f32),
            pltpu.VMEM((512, 512), f32),
        ],
        compiler_params=pltpu.CompilerParams(vmem_limit_bytes=48 << 20),
        name="attend",
    )(info, *qs, *ks, kother, wk, wv)


def per_device(
    query_main,
    query_rotary,
    latent,
    key_rotary,
    key_weight,
    value_weight,
    head_output,
    output_grad,
    row_logsum,
):
    my_z, my_x, my_c = (lax.axis_index(a) for a in SP)
    planes = lax.axis_size(Z)
    seq = (my_z + 1) // GROUP
    flags = [
        ((my_z >= s) & ((my_z - s + 1) // GROUP == seq)).astype(jnp.int32) for s in range(1, GROUP)
    ]
    info = jnp.stack([*flags, my_x, my_c]).astype(jnp.int32)
    qpack, kpack = pack(
        query_main, query_rotary, output_grad, head_output, row_logsum, latent, key_rotary
    )
    ks = [kpack] + [shift(kpack, Z, s) for s in range(1, GROUP)]
    qs = [qpack] + [shift(qpack, X, s) for s in range(1, GROUP)]
    kother = shift(jnp.stack(ks), C, 1)
    *dqs, own, other, weight = attend(info, qs, ks, kother, key_weight, value_weight)
    back = [dqs[0]] + [shift(dqs[s], X, -s) for s in range(1, GROUP)]
    grad_query = (back[0] + back[1]) + (back[2] + back[3])
    keys = own + shift(other, C, 1)
    keys = exchange(keys, Y).reshape(4, GROUP, 144, 128).sum(axis=0)
    key_t = keys[0]
    for s in range(1, GROUP):
        key_t = key_t + shift(keys[s], Z, -s)
    key_t = exchange(jnp.broadcast_to(key_t[None], (4, 144, 128)), Y)
    grad_key = key_t.reshape(576, 128).T
    weight = weight.reshape(planes, 4, 2, 4, 512)
    mine = lax.dynamic_index_in_dim(weight, my_c, 2, keepdims=False)
    theirs = lax.dynamic_index_in_dim(weight, 1 - my_c, 2, keepdims=False)
    weight = mine + shift(theirs, C, 1)
    weight = exchange(jnp.moveaxis(weight, 1, 0), X).sum(axis=0)
    near = [[a * 4 + b for b in range(4)] for a in range(planes // 4)]
    far = [[a * 4 + b for a in range(4)] for b in range(planes // 4)]
    weight = exchange(jnp.moveaxis(weight.reshape(4, 4, 4, 512), 1, 0), Z, near).sum(axis=0)
    weight = exchange(weight, Z, far).sum(axis=0)
    return (
        grad_query[:, 0:512],
        grad_query[:, 512:768],
        grad_key[:, 0:512],
        grad_key[:, 512:576],
        weight,
    )


def solution(mesh):
    finer = Mesh(mesh.devices.reshape(16, 4, 2, mesh.shape["tp"]), (Z, X, C, Y))
    return jax.shard_map(
        per_device,
        mesh=finer,
        in_specs=(
            P(SP, "tp"),
            P(SP, "tp"),
            P(SP, None),
            P(SP, None),
            P(None, "tp"),
            P(None, "tp"),
            P(SP, "tp"),
            P(SP, "tp"),
            P("tp", SP),
        ),
        out_specs=(P(SP, "tp"), P(SP, "tp"), P(SP, None), P(SP, None), P(SP, "tp")),
        check_vma=False,
    )
```

```python
import jax
import jax.numpy as jnp
from jax import lax
from jax.experimental import pallas as pl
from jax.experimental.pallas import tpu as pltpu
from jax.sharding import Mesh
from jax.sharding import PartitionSpec as P


Z, X, C, Y = "sp_0", "sp_1", "sp_2", "tp"
SP = (Z, X, C)
GROUP = 4
bf16 = jnp.bfloat16
f32 = jnp.float32


def shift(block, axis, by):
    peers = lax.axis_size(axis)
    return lax.ppermute(block, axis, [(i, (i + by) % peers) for i in range(peers)])


def onward(block, by):
    planes = lax.axis_size(Z)
    ends = [(i, i + by) for i in range(planes)]
    pairs = [(i, j) for i, j in ends if 0 <= j < planes and (i + 1) // GROUP == (j + 1) // GROUP]
    return lax.ppermute(block, Z, pairs)


def dot(a, b, dims):
    return lax.dot_general(a, b, (dims, ((), ())), preferred_element_type=f32)


def pack_kernel(qm, qr, og, ho, logs, lat, rot, qpack, kpack):
    heads, toks = logs.shape
    width = qm.shape[1] // heads
    lane = lax.broadcasted_iota(jnp.int32, (toks, 128), 1)
    extra = jnp.zeros((toks, 128), f32)
    logs_t = logs[...].T
    for h in range(heads):
        cols = slice(h * width, (h + 1) * width)
        term = jnp.sum(ho[:, cols].astype(f32) * og[:, cols].astype(f32), axis=1, keepdims=True)
        for k, value in enumerate((logs_t[:, h : h + 1], term)):
            for part in range(3):
                piece = value.astype(bf16).astype(f32)
                value = value - piece
                extra = jnp.where(lane == (h * 2 + k) * 3 + part, piece, extra)
    qpack[:, 0:512] = qm[...]
    qpack[:, 512:768] = qr[...]
    qpack[:, 768:1280] = og[...]
    qpack[:, 1280:1408] = extra.astype(bf16)
    kpack[:, 0:512] = lat[...]
    kpack[:, 512:576] = rot[...].T
    kpack[:, 576:640] = jnp.zeros((toks, 64), bf16)


def pack(*args):
    toks = args[0].shape[0]
    return pl.pallas_call(
        pack_kernel,
        out_shape=(
            jax.ShapeDtypeStruct((toks, 1408), bf16),
            jax.ShapeDtypeStruct((toks, 640), bf16),
        ),
        name="pack",
    )(*args)


def attend_kernel(
    info, q0, q1, q2, q3, k0, k1, k2, k3, kother, wk, wv,
    back, mine, theirs,
    qcur, kcur, q_s, qt_s, g_s, gt_s, log_s, term_s, acc, ds_acc, w_acc, wt_acc, back_s,
):
    heads, toks, width = 4, 128, 128
    factor = 192.0**-0.5
    my_x = info[3]
    my_c = info[4]
    ds_acc[...] = jnp.zeros_like(ds_acc)
    w_acc[...] = jnp.zeros_like(w_acc)
    wt_acc[...] = jnp.zeros_like(wt_acc)
    q_s[:, 576:640] = jnp.zeros((heads * toks, 64), bf16)

    def chunk(g, _):
        for i, ref in enumerate((q0, q1, q2, q3)):

            @pl.when(g == i)
            def _(ref=ref):
                qcur[...] = ref[...]

        extra = qcur[:, 1280:1408].astype(f32)
        for h in range(heads):
            rows = slice(h * toks, (h + 1) * toks)
            cols = slice(h * width, (h + 1) * width)
            qm_h = qcur[:, cols]
            og_h = qcur[:, 768 + h * width : 768 + (h + 1) * width]
            qr_h = qcur[:, 512 + h * 64 : 512 + (h + 1) * 64]
            q_s[rows, 0:512] = dot(qm_h, wk[:, cols], ((1,), (1,))).astype(bf16)
            qt_s[0:512, rows] = dot(wk[:, cols], qm_h, ((1,), (1,))).astype(bf16)
            g_s[rows, :] = dot(og_h, wv[:, cols], ((1,), (1,))).astype(bf16)
            gt_s[:, rows] = dot(wv[:, cols], og_h, ((1,), (1,))).astype(bf16)
            q_s[rows, 512:576] = qr_h
            qt_s[512:576, rows] = qr_h.T
            for k, ref in enumerate((log_s, term_s)):
                at = (h * 2 + k) * 3
                value = extra[:, at : at + 1] + extra[:, at + 1 : at + 2] + extra[:, at + 2 : at + 3]
                ref[rows, :] = jnp.broadcast_to(value, (toks, 128))
        acc[...] = jnp.zeros_like(acc)
        from_x = (my_x - g + GROUP) % GROUP

        def plane(p, _):
            useful = jnp.where(p == 0, from_x >= my_x, info[jnp.maximum(p - 1, 0)] == 1)

            @pl.when(useful)
            def _():
                for i, ref in enumerate((k0, k1, k2, k3)):

                    @pl.when(p == i)
                    def _(ref=ref):
                        kcur[0:toks, :] = ref[...]

                kcur[toks : 2 * toks, :] = kother[p]
                scores = dot(q_s[...], kcur[...], ((1,), (1,)))
                slopes = dot(g_s[...], kcur[:, 0:512], ((1,), (1,)))
                logs = jnp.concatenate([log_s[...]] * 2, axis=1)
                terms = jnp.concatenate([term_s[...]] * 2, axis=1)
                shape = scores.shape
                row = lax.broadcasted_iota(jnp.int32, shape, 0) % toks
                col = lax.broadcasted_iota(jnp.int32, shape, 1)
                key_c = jnp.where(col < toks, my_c, 1 - my_c)
                key_place = (my_x * 2 + key_c) * toks + col % toks
                query_place = (from_x * 2 + my_c) * toks + row
                query_place = query_place + jnp.where(p == 0, 0, 1 << 20)
                weights = jnp.where(key_place <= query_place, jnp.exp(factor * scores - logs), 0.0)
                dscores = (weights * (slopes - terms)).astype(bf16)
                acc[...] += dot(dscores, kcur[...], ((1,), (0,)))
                ds_acc[p] += dot(qt_s[...], dscores, ((1,), (0,)))
                w_acc[p] += dot(gt_s[...], weights.astype(bf16), ((1,), (0,)))

            return 0

        lax.fori_loop(0, GROUP, plane, 0)
        mains, rots = [], []
        for h in range(heads):
            rows = slice(h * toks, (h + 1) * toks)
            cols = slice(h * width, (h + 1) * width)
            mixed = acc[rows, 0:512]
            high = mixed.astype(bf16)
            low = (mixed - high.astype(f32)).astype(bf16)
            w_h = wk[:, cols]
            mains.append(factor * (dot(high, w_h, ((1,), (0,))) + dot(low, w_h, ((1,), (0,)))))
            rots.append(factor * acc[rows, 512:576])
            qm_h = qcur[:, cols]
            wt_acc[cols, :] += dot(qm_h, high, ((0,), (0,))) + dot(qm_h, low, ((0,), (0,)))
        for h in range(heads):
            back_s[from_x, h * toks : (h + 1) * toks, :] = mains[h]
        for h in range(2):
            pair = jnp.concatenate(rots[2 * h : 2 * h + 2], axis=1)
            back_s[from_x, (heads + h) * toks : (heads + h + 1) * toks, :] = pair
        return 0

    lax.fori_loop(0, GROUP, chunk, 0)
    for p in range(GROUP):
        for rows in (slice(0, 512), slice(512, 576)):
            both = factor * ds_acc[p, rows, :]
            if rows.start == 0:
                both = both + w_acc[p]
            mine[p, rows, :] = both[:, 0:toks]
            theirs[p, rows, :] = both[:, toks : 2 * toks]
    wt_acc[...] = factor * wt_acc[...].T
    upper = lax.broadcasted_iota(jnp.int32, (8, 512), 0) < 4
    for x in range(4):
        for b in range(4):
            for pair in range(2):
                one, two = (
                    wt_acc[(((8 * pair + 4 * g + b + 15) % 16) * 4 + x) * 8 :][:8] for g in range(2)
                )
                even = jnp.where(upper, one, pltpu.roll(two, 4, 0))
                odd = jnp.where(upper, pltpu.roll(one, 4, 0), two)
                at = 768 + (b * 2 + pair) * 32
                for first, tile in enumerate(
                    (jnp.where(my_c == 0, even, odd), jnp.where(my_c == 0, odd, even))
                ):
                    for k in range(4):
                        lanes = slice(k * 128, (k + 1) * 128)
                        rows = slice(at + first * 256 + k * 8, at + first * 256 + k * 8 + 8)
                        back_s[x, rows, :] = tile[:, lanes]
    back[...] = back_s[...].astype(bf16)


def attend(info, qs, ks, kother, wk, wv):
    toks = 128
    out = jax.ShapeDtypeStruct
    vmem = pl.BlockSpec(memory_space=pltpu.VMEM)
    return pl.pallas_call(
        attend_kernel,
        in_specs=[pl.BlockSpec(memory_space=pltpu.SMEM)] + [vmem] * 11,
        out_specs=[vmem] * 3,
        out_shape=[
            out((4, 1280, 128), bf16),
            out((GROUP, 576, toks), f32),
            out((GROUP, 576, toks), f32),
        ],
        scratch_shapes=[
            pltpu.VMEM((toks, 1408), bf16),
            pltpu.VMEM((2 * toks, 640), bf16),
            pltpu.VMEM((512, 640), bf16),
            pltpu.VMEM((576, 512), bf16),
            pltpu.VMEM((512, 512), bf16),
            pltpu.VMEM((512, 512), bf16),
            pltpu.VMEM((512, 128), f32),
            pltpu.VMEM((512, 128), f32),
            pltpu.VMEM((512, 640), f32),
            pltpu.VMEM((GROUP, 576, 2 * toks), f32),
            pltpu.VMEM((GROUP, 512, 2 * toks), f32),
            pltpu.VMEM((512, 512), f32),
            pltpu.VMEM((4, 1280, 128), f32),
        ],
        compiler_params=pltpu.CompilerParams(vmem_limit_bytes=60 << 20),
        name="attend",
    )(info, *qs, *ks, kother, wk, wv)


def local(body, shapes, *args, scalars=0, scratch=(), aliases=None):
    vmem = pl.BlockSpec(memory_space=pltpu.VMEM)
    smem = pl.BlockSpec(memory_space=pltpu.SMEM)
    return pl.pallas_call(
        body,
        in_specs=[smem] * scalars + [vmem] * (len(args) - scalars),
        out_specs=[vmem] * len(shapes),
        out_shape=[jax.ShapeDtypeStruct(s, t) for s, t in shapes],
        scratch_shapes=list(scratch),
        input_output_aliases=aliases or {},
        compiler_params=pltpu.CompilerParams(vmem_limit_bytes=4 << 20),
    )(*args)


def stack_kernel(k0, k1, k2, k3, out):
    for i, k in enumerate((k0, k1, k2, k3)):
        out[i] = k[...]


def pair_kernel(mine, theirs, z0, z1, z2, z3):
    for p, out in enumerate((z0, z1, z2, z3)):
        out[...] = (mine[p] + theirs[p]).astype(out.dtype)


def added(parts):
    return (parts[0] + parts[1]) + (parts[2] + parts[3])


def back_kernel(back, main, rotary, mine, theirs):
    def rows(start, count):
        return added([back[i, start : start + count, :].astype(f32) for i in range(4)])

    for h in range(4):
        main[:, h * 128 : (h + 1) * 128] = rows(h * 128, 128)
    for h in range(2):
        rotary[:, h * 128 : (h + 1) * 128] = rows(512 + h * 128, 128)
    for b in range(4):
        mine[b] = rows(768 + b * 64, 64)
        theirs[b] = rows(1024 + b * 64, 64)


def weight_kernel(mine, theirs, total):
    total[...] = mine[...] + theirs[...]


def key_kernel(z0, z1, z2, z3, key):
    key[...] = added([z[...].astype(f32) for z in (z0, z1, z2, z3)])


def far_kernel(near, far):
    total = added([near[i] for i in range(4)])
    for pair in range(2):
        for k in range(4):
            tile = total[pair * 32 + k * 8 :][:8]
            far[2 * pair, k * 8 : k * 8 + 8, :] = tile
            far[2 * pair + 1, k * 8 : k * 8 + 8, :] = pltpu.roll(tile, 4, 0)


def last_kernel(info, a0, a1, a2, a3, far, lat, rot, weight, keys):
    for s, a in enumerate((a0, a1, a2, a3)):
        keys[(info[6] - s + 4) % 4] = a[...]
    total = added([keys[y] for y in range(4)])
    lat[...] = total[0:512, :].T
    rot[...] = total[512:576, :]
    for k in range(4):
        part = added([far[i, k * 8 : k * 8 + 4, :] for i in range(4)])
        weight[:, k * 128 : (k + 1) * 128] = part


def exchange(tiles, axis, groups=None):
    return lax.all_to_all(tiles, axis, 0, 0, tiled=True, axis_index_groups=groups)


def spread(blocks, axis):
    got = [blocks[0]]
    for s in range(1, 4):
        got.append(shift(blocks[s], axis, s))
    return got


def per_device(
    query_main,
    query_rotary,
    latent,
    key_rotary,
    key_weight,
    value_weight,
    head_output,
    output_grad,
    row_logsum,
):
    my_z, my_x, my_c = (lax.axis_index(a) for a in SP)
    planes = lax.axis_size(Z)
    seq = (my_z + 1) // GROUP
    flags = [
        ((my_z >= s) & ((my_z - s + 1) // GROUP == seq)).astype(jnp.int32) for s in range(1, GROUP)
    ]
    turns = [my_x, my_c, (my_z + 1) % GROUP, lax.axis_index(Y), seq % 4]
    info = jnp.stack([*flags, *turns]).astype(jnp.int32)
    qpack, kpack = pack(
        query_main, query_rotary, output_grad, head_output, row_logsum, latent, key_rotary.T
    )
    ks = [kpack]
    for s in range(1, GROUP):
        ks.append(onward(kpack, s))
    qs = spread([qpack] * 4, X)
    (stacked,) = local(stack_kernel, [((4, *kpack.shape), bf16)], *ks)
    kother = shift(stacked, C, 1)
    back, mine, theirs = attend(info, qs, ks, kother, key_weight, value_weight)
    back = exchange(back, X)
    theirs = shift(theirs, C, 1)
    shapes = [((576, 128), f32)] + [((576, 128), bf16)] * 3
    planes = local(pair_kernel, shapes, mine, theirs)
    planes = list(planes)
    for s in range(1, 4):
        planes[s] = onward(planes[s], -s)
    toks = key_rotary.shape[0]
    shapes = [((toks, 512), f32), ((toks, 256), f32)] + [((4, 64, 128), f32)] * 2
    main, rotary, mine, theirs = local(back_kernel, shapes, back)
    theirs = shift(theirs, C, 1)
    (weight,) = local(weight_kernel, [((4, 64, 128), f32)], mine, theirs)
    near = [[(4 * g + b - 1) % 16 for b in range(4)] for g in range(4)]
    weight = exchange(weight, Z, near)
    (key,) = local(key_kernel, [((576, 128), f32)], *planes)
    keys = spread([key] * 4, Y)
    (weight,) = local(far_kernel, [((4, 32, 128), f32)], weight)
    weight = exchange(weight, Z, [list(z) for z in zip(*near)])
    shapes = [((toks, 512), f32), ((64, toks), f32), ((4, 512), f32)]
    lat, rot, weight = local(
        last_kernel, shapes, info, *keys, weight,
        scalars=1, scratch=[pltpu.VMEM((4, 576, 128), f32)],
    )
    return main, rotary, lat, rot.T, weight


def solution(mesh):
    finer = Mesh(mesh.devices.reshape(16, 4, 2, mesh.shape["tp"]), (Z, X, C, Y))
    return jax.shard_map(
        per_device,
        mesh=finer,
        in_specs=(
            P(SP, "tp"),
            P(SP, "tp"),
            P(SP, None),
            P(SP, None),
            P(None, "tp"),
            P(None, "tp"),
            P(SP, "tp"),
            P(SP, "tp"),
            P("tp", SP),
        ),
        out_specs=(P(SP, "tp"), P(SP, "tp"), P(SP, None), P(SP, None), P(SP, "tp")),
        check_vma=False,
    )
```

```python
import jax
import jax.numpy as jnp
from jax import lax
from jax.experimental import pallas as pl
from jax.experimental.pallas import tpu as pltpu
from jax.sharding import Mesh
from jax.sharding import PartitionSpec as P


Z, X, C, Y = "sp_0", "sp_1", "sp_2", "tp"
SP = (Z, X, C)
GROUP = 4
bf16 = jnp.bfloat16
f32 = jnp.float32


def shift(block, axis, by):
    peers = lax.axis_size(axis)
    return lax.ppermute(block, axis, [(i, (i + by) % peers) for i in range(peers)])


def onward(block, by):
    planes = lax.axis_size(Z)
    ends = [(i, i + by) for i in range(planes)]
    pairs = [(i, j) for i, j in ends if 0 <= j < planes and (i + 1) // GROUP == (j + 1) // GROUP]
    return lax.ppermute(block, Z, pairs)


def dot(a, b, dims):
    return lax.dot_general(a, b, (dims, ((), ())), preferred_element_type=f32)


def pack_kernel(qm, qr, og, ho, logs, lat, rot, qpack, kpack):
    heads, toks = logs.shape
    width = qm.shape[1] // heads
    lane = lax.broadcasted_iota(jnp.int32, (toks, 128), 1)
    extra = jnp.zeros((toks, 128), f32)
    logs_t = logs[...].T
    for h in range(heads):
        cols = slice(h * width, (h + 1) * width)
        term = jnp.sum(ho[:, cols].astype(f32) * og[:, cols].astype(f32), axis=1, keepdims=True)
        for k, value in enumerate((logs_t[:, h : h + 1], term)):
            for part in range(3):
                piece = value.astype(bf16).astype(f32)
                value = value - piece
                extra = jnp.where(lane == (h * 2 + k) * 3 + part, piece, extra)
    for i in range(qpack.shape[0]):
        qpack[i, :, 0:512] = qm[...]
        qpack[i, :, 512:768] = qr[...]
        qpack[i, :, 768:1280] = og[...]
        qpack[i, :, 1280:1408] = extra.astype(bf16)
    kpack[:, 0:512] = lat[...]
    kpack[:, 512:576] = rot[...].T
    kpack[:, 576:640] = jnp.zeros((toks, 64), bf16)


def pack(*args):
    toks = args[0].shape[0]
    return pl.pallas_call(
        pack_kernel,
        out_shape=(
            jax.ShapeDtypeStruct((4, toks, 1408), bf16),
            jax.ShapeDtypeStruct((toks, 640), bf16),
        ),
        name="pack",
    )(*args)


def attend_kernel(
    info, qs, k0, k1, k2, k3, kother, wk, wv,
    back, mine, theirs,
    kcur, q_s, qt_s, g_s, gt_s, log_s, term_s, gap_s, acc, ds_acc, w_acc, wt_acc, back_s,
):
    heads, toks, width = 4, 128, 128
    factor = 192.0**-0.5
    my_x = info[3]
    my_c = info[4]

    def whole(start, count):
        return qs[:, :, start : start + count].reshape(GROUP * toks, count)

    acc[...] = jnp.zeros_like(acc)
    ds_acc[...] = jnp.zeros_like(ds_acc)
    w_acc[...] = jnp.zeros_like(w_acc)
    shape = (2 * toks, 2 * toks)
    gap_s[...] = (
        lax.broadcasted_iota(jnp.int32, shape, 1) % toks
        - lax.broadcasted_iota(jnp.int32, shape, 0) % toks
    )
    for i in range(GROUP):
        q_s[i, :, 576:640] = jnp.zeros((heads * toks, 64), bf16)
    for h in range(heads):
        rows = slice(h * toks, (h + 1) * toks)
        cols = slice(h * width, (h + 1) * width)
        for at, w, plain, turned in ((0, wk, q_s, qt_s), (768, wv, g_s, gt_s)):
            x_h = whole(at + h * width, width)
            w_h = w[:, cols]
            straight = dot(x_h, w_h, ((1,), (1,))).astype(bf16)
            across = dot(w_h, x_h, ((1,), (1,))).astype(bf16)
            for i in range(GROUP):
                plain[i, rows, 0:512] = straight[i * toks : (i + 1) * toks, :]
                turned[i, 0:512, rows] = across[:, i * toks : (i + 1) * toks]
        for i in range(GROUP):
            qr_h = qs[i, :, 512 + h * 64 : 512 + (h + 1) * 64]
            q_s[i, rows, 512:576] = qr_h
            qt_s[i, 512:576, rows] = qr_h.T
            extra = qs[i, :, 1280:1408].astype(f32)
            for k, ref in enumerate((log_s, term_s)):
                at = (h * 2 + k) * 3
                value = extra[:, at : at + 1] + extra[:, at + 1 : at + 2] + extra[:, at + 2 : at + 3]
                ref[i, rows, :] = jnp.broadcast_to(value, (toks, 128))

    own_key = lax.broadcasted_iota(jnp.int32, (1, 2 * toks), 1) < toks
    key_c = jnp.where(own_key, my_c, 1 - my_c)

    def plane(p, _):
        @pl.when((p == 0) | (info[jnp.maximum(p - 1, 0)] == 1))
        def _():
            for i, ref in enumerate((k0, k1, k2, k3)):

                @pl.when(p == i)
                def _(ref=ref):
                    kcur[0:toks, :] = ref[...]

            kcur[toks : 2 * toks, :] = kother[p]

            def chunk(i, _):
                ahead = ((i - my_x) * 2 + my_c - key_c) * toks
                limit = ahead + jnp.where(p == 0, 0, 1 << 20)
                lows, slopes_low = [], []
                for half in range(2):
                    rows = slice(half * 2 * toks, (half + 1) * 2 * toks)
                    scores = dot(q_s[i, rows, :], kcur[...], ((1,), (1,)))
                    slopes = dot(g_s[i, rows, :], kcur[:, 0:512], ((1,), (1,)))
                    logs = jnp.concatenate([log_s[i, rows, :]] * 2, axis=1)
                    terms = jnp.concatenate([term_s[i, rows, :]] * 2, axis=1)
                    weights = jnp.exp(factor * scores - logs)
                    weights = jnp.where(gap_s[...] <= limit, weights, 0.0)
                    dscores = (weights * (slopes - terms)).astype(bf16)
                    acc[i, rows, :] += dot(dscores, kcur[...], ((1,), (0,)))
                    lows.append(weights.astype(bf16))
                    slopes_low.append(dscores)
                ds_acc[p] += dot(qt_s[i], jnp.concatenate(slopes_low, axis=0), ((1,), (0,)))
                w_acc[p] += dot(gt_s[i], jnp.concatenate(lows, axis=0), ((1,), (0,)))
                return 0

            lax.fori_loop(jnp.where(p == 0, my_x, 0), GROUP, chunk, 0)

        return 0

    lax.fori_loop(0, GROUP, plane, 0)
    for h in range(heads):
        rows = slice(h * toks, (h + 1) * toks)
        cols = slice(h * width, (h + 1) * width)
        mixed = acc[:, rows, 0:512].reshape(GROUP * toks, 512)
        high = mixed.astype(bf16)
        low = (mixed - high.astype(f32)).astype(bf16)
        w_h = wk[:, cols]
        main = factor * (dot(high, w_h, ((1,), (0,))) + dot(low, w_h, ((1,), (0,))))
        x_h = whole(h * width, width)
        wt_acc[cols, :] = dot(x_h, high, ((0,), (0,))) + dot(x_h, low, ((0,), (0,)))
        for i in range(GROUP):
            back_s[i, rows, :] = main[i * toks : (i + 1) * toks, :]
    for i in range(GROUP):
        for h in range(2):
            pair = [acc[i, (2 * h + k) * toks : (2 * h + k + 1) * toks, 512:576] for k in range(2)]
            rows = slice((heads + h) * toks, (heads + h + 1) * toks)
            back_s[i, rows, :] = factor * jnp.concatenate(pair, axis=1)
    for p in range(GROUP):
        for rows in (slice(0, 512), slice(512, 576)):
            both = factor * ds_acc[p, rows, :]
            if rows.start == 0:
                both = both + w_acc[p]
            mine[p, rows, :] = both[:, 0:toks]
            theirs[p, rows, :] = both[:, toks : 2 * toks]
    wt_acc[...] = factor * wt_acc[...].T
    upper = lax.broadcasted_iota(jnp.int32, (8, 512), 0) < 4
    for x in range(4):
        for b in range(4):
            for pair in range(2):
                one, two = (
                    wt_acc[(((8 * pair + 4 * g + b + 15) % 16) * 4 + x) * 8 :][:8] for g in range(2)
                )
                even = jnp.where(upper, one, pltpu.roll(two, 4, 0))
                odd = jnp.where(upper, pltpu.roll(one, 4, 0), two)
                at = 768 + (b * 2 + pair) * 32
                for first, tile in enumerate(
                    (jnp.where(my_c == 0, even, odd), jnp.where(my_c == 0, odd, even))
                ):
                    for k in range(4):
                        lanes = slice(k * 128, (k + 1) * 128)
                        rows = slice(at + first * 256 + k * 8, at + first * 256 + k * 8 + 8)
                        back_s[x, rows, :] = tile[:, lanes]
    back[...] = back_s[...].astype(bf16)


def attend(info, qs, ks, kother, wk, wv):
    toks = 128
    out = jax.ShapeDtypeStruct
    vmem = pl.BlockSpec(memory_space=pltpu.VMEM)
    return pl.pallas_call(
        attend_kernel,
        in_specs=[pl.BlockSpec(memory_space=pltpu.SMEM)] + [vmem] * 8,
        out_specs=[vmem] * 3,
        out_shape=[
            out((4, 1280, 128), bf16),
            out((GROUP, 576, toks), f32),
            out((GROUP, 576, toks), f32),
        ],
        scratch_shapes=[
            pltpu.VMEM((2 * toks, 640), bf16),
            pltpu.VMEM((GROUP, 512, 640), bf16),
            pltpu.VMEM((GROUP, 576, 512), bf16),
            pltpu.VMEM((GROUP, 512, 512), bf16),
            pltpu.VMEM((GROUP, 512, 512), bf16),
            pltpu.VMEM((GROUP, 512, 128), f32),
            pltpu.VMEM((GROUP, 512, 128), f32),
            pltpu.VMEM((2 * toks, 2 * toks), jnp.int32),
            pltpu.VMEM((GROUP, 512, 640), f32),
            pltpu.VMEM((GROUP, 576, 2 * toks), f32),
            pltpu.VMEM((GROUP, 512, 2 * toks), f32),
            pltpu.VMEM((512, 512), f32),
            pltpu.VMEM((4, 1280, 128), f32),
        ],
        compiler_params=pltpu.CompilerParams(vmem_limit_bytes=52 << 20),
        name="attend",
    )(info, qs, *ks, kother, wk, wv)


def local(body, shapes, *args, scalars=0, scratch=(), aliases=None):
    vmem = pl.BlockSpec(memory_space=pltpu.VMEM)
    smem = pl.BlockSpec(memory_space=pltpu.SMEM)
    return pl.pallas_call(
        body,
        in_specs=[smem] * scalars + [vmem] * (len(args) - scalars),
        out_specs=[vmem] * len(shapes),
        out_shape=[jax.ShapeDtypeStruct(s, t) for s, t in shapes],
        scratch_shapes=list(scratch),
        input_output_aliases=aliases or {},
        compiler_params=pltpu.CompilerParams(vmem_limit_bytes=4 << 20),
    )(*args)


def stack_kernel(k0, k1, k2, k3, out):
    for i, k in enumerate((k0, k1, k2, k3)):
        out[i] = k[...]


def pair_kernel(mine, theirs, z0, z1, z2, z3):
    for p, out in enumerate((z0, z1, z2, z3)):
        out[...] = (mine[p] + theirs[p]).astype(out.dtype)


def added(parts):
    return (parts[0] + parts[1]) + (parts[2] + parts[3])


def back_kernel(back, main, rotary, mine, theirs):
    def rows(start, count):
        return added([back[i, start : start + count, :].astype(f32) for i in range(4)])

    for h in range(4):
        main[:, h * 128 : (h + 1) * 128] = rows(h * 128, 128)
    for h in range(2):
        rotary[:, h * 128 : (h + 1) * 128] = rows(512 + h * 128, 128)
    for b in range(4):
        mine[b] = rows(768 + b * 64, 64)
        theirs[b] = rows(1024 + b * 64, 64)


def weight_kernel(mine, theirs, total):
    total[...] = mine[...] + theirs[...]


def key_kernel(z0, z1, z2, z3, key):
    key[...] = added([z[...].astype(f32) for z in (z0, z1, z2, z3)])


def far_kernel(near, far):
    total = added([near[i] for i in range(4)])
    for pair in range(2):
        for k in range(4):
            tile = total[pair * 32 + k * 8 :][:8]
            far[2 * pair, k * 8 : k * 8 + 8, :] = tile
            far[2 * pair + 1, k * 8 : k * 8 + 8, :] = pltpu.roll(tile, 4, 0)


def last_kernel(keys, other_keys, far, lat, rot, weight):
    total = keys[...] + other_keys[...]
    lat[...] = total[0:512, :].T
    rot[...] = total[512:576, :]
    for k in range(4):
        part = added([far[i, k * 8 : k * 8 + 4, :] for i in range(4)])
        weight[:, k * 128 : (k + 1) * 128] = part


def swap(block, axis, bit):
    pairs = [(i, i ^ bit) for i in range(lax.axis_size(axis))]
    return lax.ppermute(block, axis, pairs)


def exchange(tiles, axis, groups=None):
    return lax.all_to_all(tiles, axis, 0, 0, tiled=True, axis_index_groups=groups)


def per_device(
    query_main,
    query_rotary,
    latent,
    key_rotary,
    key_weight,
    value_weight,
    head_output,
    output_grad,
    row_logsum,
):
    my_z, my_x, my_c = (lax.axis_index(a) for a in SP)
    planes = lax.axis_size(Z)
    seq = (my_z + 1) // GROUP
    flags = [
        ((my_z >= s) & ((my_z - s + 1) // GROUP == seq)).astype(jnp.int32) for s in range(1, GROUP)
    ]
    info = jnp.stack([*flags, my_x, my_c]).astype(jnp.int32)
    qpack, kpack = pack(
        query_main, query_rotary, output_grad, head_output, row_logsum, latent, key_rotary.T
    )
    ks = [kpack]
    for s in range(1, GROUP):
        ks.append(onward(kpack, s))
    qs = exchange(qpack, X)
    (stacked,) = local(stack_kernel, [((4, *kpack.shape), bf16)], *ks)
    kother = shift(stacked, C, 1)
    back, mine, theirs = attend(info, qs, ks, kother, key_weight, value_weight)
    back = exchange(back, X)
    theirs = shift(theirs, C, 1)
    shapes = [((576, 128), f32)] + [((576, 128), bf16)] * 3
    planes = local(pair_kernel, shapes, mine, theirs)
    planes = list(planes)
    for s in range(1, 4):
        planes[s] = onward(planes[s], -s)
    toks = key_rotary.shape[0]
    shapes = [((toks, 512), f32), ((toks, 256), f32)] + [((4, 64, 128), f32)] * 2
    main, rotary, mine, theirs = local(back_kernel, shapes, back)
    theirs = shift(theirs, C, 1)
    (weight,) = local(weight_kernel, [((4, 64, 128), f32)], mine, theirs)
    near = [[(4 * g + b - 1) % 16 for b in range(4)] for g in range(4)]
    weight = exchange(weight, Z, near)
    (key,) = local(key_kernel, [((576, 128), f32)], *planes)
    beside = swap(key, Y, 1)
    (key,) = local(weight_kernel, [((576, 128), f32)], key, beside)
    across = swap(key, Y, 2)
    (weight,) = local(far_kernel, [((4, 32, 128), f32)], weight)
    weight = exchange(weight, Z, [list(z) for z in zip(*near)])
    shapes = [((toks, 512), f32), ((64, toks), f32), ((4, 512), f32)]
    lat, rot, weight = local(last_kernel, shapes, key, across, weight)
    return main, rotary, lat, rot.T, weight


def solution(mesh):
    finer = Mesh(mesh.devices.reshape(16, 4, 2, mesh.shape["tp"]), (Z, X, C, Y))
    return jax.shard_map(
        per_device,
        mesh=finer,
        in_specs=(
            P(SP, "tp"),
            P(SP, "tp"),
            P(SP, None),
            P(SP, None),
            P(None, "tp"),
            P(None, "tp"),
            P(SP, "tp"),
            P(SP, "tp"),
            P("tp", SP),
        ),
        out_specs=(P(SP, "tp"), P(SP, "tp"), P(SP, None), P(SP, None), P(SP, "tp")),
        check_vma=False,
    )
```

```python
import jax
import jax.numpy as jnp
from jax import lax
from jax.experimental import pallas as pl
from jax.experimental.pallas import tpu as pltpu
from jax.sharding import Mesh
from jax.sharding import PartitionSpec as P


Z, X, C, Y = "sp_0", "sp_1", "sp_2", "tp"
SP = (Z, X, C)
GROUP = 4
bf16 = jnp.bfloat16
f32 = jnp.float32


def shift(block, axis, by):
    peers = lax.axis_size(axis)
    return lax.ppermute(block, axis, [(i, (i + by) % peers) for i in range(peers)])


def onward(block, by):
    planes = lax.axis_size(Z)
    ends = [(i, i + by) for i in range(planes)]
    pairs = [(i, j) for i, j in ends if 0 <= j < planes and (i + 1) // GROUP == (j + 1) // GROUP]
    return lax.ppermute(block, Z, pairs)


def dot(a, b, dims):
    return lax.dot_general(a, b, (dims, ((), ())), preferred_element_type=f32)


def pack_kernel(qm, qr, og, ho, logs, lat, rot, qpack, kpack):
    heads, toks = logs.shape
    width = qm.shape[1] // heads
    lane = lax.broadcasted_iota(jnp.int32, (toks, 128), 1)
    extra = jnp.zeros((toks, 128), f32)
    logs_t = logs[...].T
    for h in range(heads):
        cols = slice(h * width, (h + 1) * width)
        term = jnp.sum(ho[:, cols].astype(f32) * og[:, cols].astype(f32), axis=1, keepdims=True)
        for k, value in enumerate((logs_t[:, h : h + 1], term)):
            for part in range(3):
                piece = value.astype(bf16).astype(f32)
                value = value - piece
                extra = jnp.where(lane == (h * 2 + k) * 3 + part, piece, extra)
    for i in range(qpack.shape[0]):
        qpack[i, :, 0:512] = qm[...]
        qpack[i, :, 512:768] = qr[...]
        qpack[i, :, 768:1280] = og[...]
        qpack[i, :, 1280:1408] = extra.astype(bf16)
    kpack[:, 0:512] = lat[...]
    kpack[:, 512:576] = rot[...].T
    kpack[:, 576:640] = jnp.zeros((toks, 64), bf16)


def pack(*args):
    toks = args[0].shape[0]
    return pl.pallas_call(
        pack_kernel,
        out_shape=(
            jax.ShapeDtypeStruct((4, toks, 1408), bf16),
            jax.ShapeDtypeStruct((toks, 640), bf16),
        ),
        name="pack",
    )(*args)


def attend_kernel(
    info, qs, k0, k1, k2, k3, kother, wk, wv,
    back, mine, theirs,
    kcur, q_s, qt_s, g_s, gt_s, log_s, term_s, gap_s, acc, ds_acc, w_acc, wt_acc, back_s,
):
    heads, toks, width = 4, 128, 128
    factor = 192.0**-0.5
    my_x = info[3]
    my_c = info[4]

    def whole(start, count):
        return qs[:, :, start : start + count].reshape(GROUP * toks, count)

    acc[...] = jnp.zeros_like(acc)
    ds_acc[...] = jnp.zeros_like(ds_acc)
    w_acc[...] = jnp.zeros_like(w_acc)
    shape = (2 * toks, 2 * toks)
    gap_s[...] = (
        lax.broadcasted_iota(jnp.int32, shape, 1) % toks
        - lax.broadcasted_iota(jnp.int32, shape, 0) % toks
    )
    for i in range(GROUP):
        q_s[i, :, 576:640] = jnp.zeros((heads * toks, 64), bf16)
    for h in range(heads):
        rows = slice(h * toks, (h + 1) * toks)
        cols = slice(h * width, (h + 1) * width)
        for at, w, plain, turned in ((0, wk, q_s, qt_s), (768, wv, g_s, gt_s)):
            x_h = whole(at + h * width, width)
            w_h = w[:, cols]
            straight = dot(x_h, w_h, ((1,), (1,))).astype(bf16)
            across = dot(w_h, x_h, ((1,), (1,))).astype(bf16)
            for i in range(GROUP):
                plain[i, rows, 0:512] = straight[i * toks : (i + 1) * toks, :]
                turned[i, 0:512, rows] = across[:, i * toks : (i + 1) * toks]
        for i in range(GROUP):
            qr_h = qs[i, :, 512 + h * 64 : 512 + (h + 1) * 64]
            q_s[i, rows, 512:576] = qr_h
            qt_s[i, 512:576, rows] = qr_h.T
            extra = qs[i, :, 1280:1408].astype(f32)
            for k, ref in enumerate((log_s, term_s)):
                at = (h * 2 + k) * 3
                value = extra[:, at : at + 1] + extra[:, at + 1 : at + 2] + extra[:, at + 2 : at + 3]
                ref[i, rows, :] = jnp.broadcast_to(value, (toks, 128))

    own_key = lax.broadcasted_iota(jnp.int32, (1, 2 * toks), 1) < toks
    key_c = jnp.where(own_key, my_c, 1 - my_c)

    def plane(p, _):
        @pl.when((p == 0) | (info[jnp.maximum(p - 1, 0)] == 1))
        def _():
            for i, ref in enumerate((k0, k1, k2, k3)):

                @pl.when(p == i)
                def _(ref=ref):
                    kcur[0:toks, :] = ref[...]

            kcur[toks : 2 * toks, :] = kother[p]

            def chunk(i, _):
                ahead = ((i - my_x) * 2 + my_c - key_c) * toks
                limit = ahead + jnp.where(p == 0, 0, 1 << 20)
                lows, slopes_low = [], []
                for half in range(2):
                    rows = slice(half * 2 * toks, (half + 1) * 2 * toks)
                    scores = dot(q_s[i, rows, :], kcur[...], ((1,), (1,)))
                    slopes = dot(g_s[i, rows, :], kcur[:, 0:512], ((1,), (1,)))
                    logs = jnp.concatenate([log_s[i, rows, :]] * 2, axis=1)
                    terms = jnp.concatenate([term_s[i, rows, :]] * 2, axis=1)
                    weights = jnp.exp(factor * scores - logs)
                    weights = jnp.where(gap_s[...] <= limit, weights, 0.0)
                    dscores = (weights * (slopes - terms)).astype(bf16)
                    acc[i, rows, :] += dot(dscores, kcur[...], ((1,), (0,)))
                    lows.append(weights.astype(bf16))
                    slopes_low.append(dscores)
                ds_acc[p] += dot(qt_s[i], jnp.concatenate(slopes_low, axis=0), ((1,), (0,)))
                w_acc[p] += dot(gt_s[i], jnp.concatenate(lows, axis=0), ((1,), (0,)))
                return 0

            lax.fori_loop(jnp.where(p == 0, my_x, 0), GROUP, chunk, 0)

        return 0

    lax.fori_loop(0, GROUP, plane, 0)
    for h in range(heads):
        rows = slice(h * toks, (h + 1) * toks)
        cols = slice(h * width, (h + 1) * width)
        mixed = acc[:, rows, 0:512].reshape(GROUP * toks, 512)
        high = mixed.astype(bf16)
        low = (mixed - high.astype(f32)).astype(bf16)
        w_h = wk[:, cols]
        main = factor * (dot(high, w_h, ((1,), (0,))) + dot(low, w_h, ((1,), (0,))))
        x_h = whole(h * width, width)
        wt_acc[cols, :] = dot(x_h, high, ((0,), (0,))) + dot(x_h, low, ((0,), (0,)))
        for i in range(GROUP):
            back_s[i, rows, :] = main[i * toks : (i + 1) * toks, :]
    for i in range(GROUP):
        for h in range(2):
            pair = [acc[i, (2 * h + k) * toks : (2 * h + k + 1) * toks, 512:576] for k in range(2)]
            rows = slice((heads + h) * toks, (heads + h + 1) * toks)
            back_s[i, rows, :] = factor * jnp.concatenate(pair, axis=1)
    for p in range(GROUP):
        for rows in (slice(0, 512), slice(512, 576)):
            both = factor * ds_acc[p, rows, :]
            if rows.start == 0:
                both = both + w_acc[p]
            mine[p, rows, :] = both[:, 0:toks]
            theirs[p, rows, :] = both[:, toks : 2 * toks]
    wt_acc[...] = factor * wt_acc[...].T
    upper = lax.broadcasted_iota(jnp.int32, (8, 512), 0) < 4
    for x in range(4):
        for b in range(4):
            for pair in range(2):
                one, two = (
                    wt_acc[(((8 * pair + 4 * g + b + 15) % 16) * 4 + x) * 8 :][:8] for g in range(2)
                )
                even = jnp.where(upper, one, pltpu.roll(two, 4, 0))
                odd = jnp.where(upper, pltpu.roll(one, 4, 0), two)
                at = 768 + (b * 2 + pair) * 32
                for first, tile in enumerate((even, odd)):
                    for k in range(4):
                        lanes = slice(k * 128, (k + 1) * 128)
                        rows = slice(at + first * 256 + k * 8, at + first * 256 + k * 8 + 8)
                        back_s[x, rows, :] = tile[:, lanes]
    back[...] = back_s[...].astype(bf16)


def attend(info, qs, ks, kother, wk, wv):
    toks = 128
    out = jax.ShapeDtypeStruct
    vmem = pl.BlockSpec(memory_space=pltpu.VMEM)
    return pl.pallas_call(
        attend_kernel,
        in_specs=[pl.BlockSpec(memory_space=pltpu.SMEM)] + [vmem] * 8,
        out_specs=[vmem] * 3,
        out_shape=[
            out((4, 1280, 128), bf16),
            out((GROUP, 576, toks), f32),
            out((GROUP, 576, toks), f32),
        ],
        scratch_shapes=[
            pltpu.VMEM((2 * toks, 640), bf16),
            pltpu.VMEM((GROUP, 512, 640), bf16),
            pltpu.VMEM((GROUP, 576, 512), bf16),
            pltpu.VMEM((GROUP, 512, 512), bf16),
            pltpu.VMEM((GROUP, 512, 512), bf16),
            pltpu.VMEM((GROUP, 512, 128), f32),
            pltpu.VMEM((GROUP, 512, 128), f32),
            pltpu.VMEM((2 * toks, 2 * toks), jnp.int32),
            pltpu.VMEM((GROUP, 512, 640), f32),
            pltpu.VMEM((GROUP, 576, 2 * toks), f32),
            pltpu.VMEM((GROUP, 512, 2 * toks), f32),
            pltpu.VMEM((512, 512), f32),
            pltpu.VMEM((4, 1280, 128), f32),
        ],
        compiler_params=pltpu.CompilerParams(vmem_limit_bytes=52 << 20),
        name="attend",
    )(info, qs, *ks, kother, wk, wv)


def local(body, shapes, *args, scalars=0, scratch=(), aliases=None):
    vmem = pl.BlockSpec(memory_space=pltpu.VMEM)
    smem = pl.BlockSpec(memory_space=pltpu.SMEM)
    return pl.pallas_call(
        body,
        in_specs=[smem] * scalars + [vmem] * (len(args) - scalars),
        out_specs=[vmem] * len(shapes),
        out_shape=[jax.ShapeDtypeStruct(s, t) for s, t in shapes],
        scratch_shapes=list(scratch),
        input_output_aliases=aliases or {},
        compiler_params=pltpu.CompilerParams(vmem_limit_bytes=4 << 20),
    )(*args)


def stack_kernel(k0, k1, k2, k3, out):
    for i, k in enumerate((k0, k1, k2, k3)):
        out[i] = k[...]


def pair_kernel(mine, theirs, z0, z1, z2, z3):
    for p, out in enumerate((z0, z1, z2, z3)):
        out[...] = (mine[p] + theirs[p]).astype(out.dtype)


def added(parts):
    return (parts[0] + parts[1]) + (parts[2] + parts[3])


def back_kernel(back, main, rotary, near):
    def rows(start, count):
        return added([back[i, start : start + count, :].astype(f32) for i in range(4)])

    for h in range(4):
        main[:, h * 128 : (h + 1) * 128] = rows(h * 128, 128)
    for h in range(2):
        rotary[:, h * 128 : (h + 1) * 128] = rows(512 + h * 128, 128)
    for b in range(4):
        for c in range(2):
            near[2 * b + c] = rows(768 + c * 256 + b * 64, 64)


def couple_kernel(mine, theirs, total):
    total[...] = (mine[...].astype(f32) + theirs[...].astype(f32)).astype(bf16)


def key_kernel(z0, z1, z2, z3, key):
    key[...] = added([z[...].astype(f32) for z in (z0, z1, z2, z3)]).astype(bf16)


def far_kernel(near, far):
    total = added([near[i] + near[i + 4] for i in range(4)])
    for pair in range(2):
        for k in range(4):
            tile = total[pair * 32 + k * 8 :][:8]
            far[2 * pair, k * 8 : k * 8 + 8, :] = tile
            far[2 * pair + 1, k * 8 : k * 8 + 8, :] = pltpu.roll(tile, 4, 0)


def last_kernel(keys, other_keys, far, lat, rot, weight):
    total = keys[...].astype(f32) + other_keys[...].astype(f32)
    lat[...] = total[0:512, :].T
    rot[...] = total[512:576, :]
    for k in range(4):
        part = added([far[i, k * 8 : k * 8 + 4, :] for i in range(4)])
        weight[:, k * 128 : (k + 1) * 128] = part


def swap(block, axis, bit):
    pairs = [(i, i ^ bit) for i in range(lax.axis_size(axis))]
    return lax.ppermute(block, axis, pairs)


def exchange(tiles, axis, groups=None):
    return lax.all_to_all(tiles, axis, 0, 0, tiled=True, axis_index_groups=groups)


def per_device(
    query_main,
    query_rotary,
    latent,
    key_rotary,
    key_weight,
    value_weight,
    head_output,
    output_grad,
    row_logsum,
):
    my_z, my_x, my_c = (lax.axis_index(a) for a in SP)
    planes = lax.axis_size(Z)
    seq = (my_z + 1) // GROUP
    flags = [
        ((my_z >= s) & ((my_z - s + 1) // GROUP == seq)).astype(jnp.int32) for s in range(1, GROUP)
    ]
    info = jnp.stack([*flags, my_x, my_c]).astype(jnp.int32)
    qpack, kpack = pack(
        query_main, query_rotary, output_grad, head_output, row_logsum, latent, key_rotary.T
    )
    ks = [kpack]
    for s in range(1, GROUP):
        ks.append(onward(kpack, s))
    qs = exchange(qpack, X)
    (stacked,) = local(stack_kernel, [((4, *kpack.shape), bf16)], *ks)
    kother = shift(stacked, C, 1)
    back, mine, theirs = attend(info, qs, ks, kother, key_weight, value_weight)
    back = exchange(back, X)
    theirs = shift(theirs, C, 1)
    shapes = [((576, 128), f32)] + [((576, 128), bf16)] * 3
    planes = local(pair_kernel, shapes, mine, theirs)
    planes = list(planes)
    for s in range(1, 4):
        planes[s] = onward(planes[s], -s)
    toks = key_rotary.shape[0]
    shapes = [((toks, 512), f32), ((toks, 256), f32), ((8, 64, 128), f32)]
    main, rotary, weight = local(back_kernel, shapes, back)
    near = [[(4 * g + b - 1) % 16 for b in range(4)] for g in range(4)]
    pairs = [[2 * z + c for z in zs for c in range(2)] for zs in near]
    weight = exchange(weight, (Z, C), pairs)
    (key,) = local(key_kernel, [((576, 128), bf16)], *planes)
    beside = swap(key, Y, 1)
    (key,) = local(couple_kernel, [((576, 128), bf16)], key, beside)
    across = swap(key, Y, 2)
    (weight,) = local(far_kernel, [((4, 32, 128), f32)], weight)
    weight = exchange(weight, Z, [list(z) for z in zip(*near)])
    shapes = [((toks, 512), f32), ((64, toks), f32), ((4, 512), f32)]
    lat, rot, weight = local(last_kernel, shapes, key, across, weight)
    return main, rotary, lat, rot.T, weight


def solution(mesh):
    finer = Mesh(mesh.devices.reshape(16, 4, 2, mesh.shape["tp"]), (Z, X, C, Y))
    return jax.shard_map(
        per_device,
        mesh=finer,
        in_specs=(
            P(SP, "tp"),
            P(SP, "tp"),
            P(SP, None),
            P(SP, None),
            P(None, "tp"),
            P(None, "tp"),
            P(SP, "tp"),
            P(SP, "tp"),
            P("tp", SP),
        ),
        out_specs=(P(SP, "tp"), P(SP, "tp"), P(SP, None), P(SP, None), P(SP, "tp")),
        check_vma=False,
    )
```

```python
import jax
import jax.numpy as jnp
from jax import lax
from jax.experimental import pallas as pl
from jax.experimental.pallas import tpu as pltpu
from jax.sharding import Mesh
from jax.sharding import PartitionSpec as P


Z, X, C, Y = "sp_0", "sp_1", "sp_2", "tp"
SP = (Z, X, C)
GROUP = 4
bf16 = jnp.bfloat16
f32 = jnp.float32


def shift(block, axis, by):
    peers = lax.axis_size(axis)
    return lax.ppermute(block, axis, [(i, (i + by) % peers) for i in range(peers)])


def onward(block, by):
    planes = lax.axis_size(Z)
    ends = [(i, i + by) for i in range(planes)]
    pairs = [(i, j) for i, j in ends if 0 <= j < planes and (i + 1) // GROUP == (j + 1) // GROUP]
    return lax.ppermute(block, Z, pairs)


def dot(a, b, dims):
    return lax.dot_general(a, b, (dims, ((), ())), preferred_element_type=f32)


def pack_kernel(qm, qr, og, ho, logs, lat, rot, qpack, kpack):
    heads, toks = logs.shape
    width = qm.shape[1] // heads
    lane = lax.broadcasted_iota(jnp.int32, (toks, 128), 1)
    extra = jnp.zeros((toks, 128), f32)
    logs_t = logs[...].T
    for h in range(heads):
        cols = slice(h * width, (h + 1) * width)
        term = jnp.sum(ho[:, cols].astype(f32) * og[:, cols].astype(f32), axis=1, keepdims=True)
        for k, value in enumerate((logs_t[:, h : h + 1], term)):
            for part in range(3):
                piece = value.astype(bf16).astype(f32)
                value = value - piece
                extra = jnp.where(lane == (h * 2 + k) * 3 + part, piece, extra)
    for i in range(qpack.shape[0]):
        qpack[i, :, 0:512] = qm[...]
        qpack[i, :, 512:768] = qr[...]
        qpack[i, :, 768:1280] = og[...]
        qpack[i, :, 1280:1408] = extra.astype(bf16)
    kpack[:, 0:512] = lat[...]
    kpack[:, 512:576] = rot[...].T
    kpack[:, 576:640] = jnp.zeros((toks, 64), bf16)


def pack(*args):
    toks = args[0].shape[0]
    return pl.pallas_call(
        pack_kernel,
        out_shape=(
            jax.ShapeDtypeStruct((4, toks, 1408), bf16),
            jax.ShapeDtypeStruct((toks, 640), bf16),
        ),
        name="pack",
    )(*args)


def attend_kernel(
    info, qs, k0, k1, k2, k3, kother, wk, wv,
    back, mine, theirs,
    kcur, q_s, qt_s, g_s, gt_s, log_s, term_s, gap_s, acc, ds_acc, w_acc, wt_acc, back_s,
):
    heads, toks, width = 4, 128, 128
    factor = 192.0**-0.5
    my_x = info[3]
    my_c = info[4]

    def whole(start, count):
        return qs[:, :, start : start + count].reshape(GROUP * toks, count)

    acc[...] = jnp.zeros_like(acc)
    ds_acc[...] = jnp.zeros_like(ds_acc)
    w_acc[...] = jnp.zeros_like(w_acc)
    shape = (heads * toks, 2 * toks)
    gap_s[...] = (
        lax.broadcasted_iota(jnp.int32, shape, 1) % toks
        - lax.broadcasted_iota(jnp.int32, shape, 0) % toks
    )
    for i in range(GROUP):
        q_s[i, :, 576:640] = jnp.zeros((heads * toks, 64), bf16)
    for h in range(heads):
        rows = slice(h * toks, (h + 1) * toks)
        cols = slice(h * width, (h + 1) * width)
        for at, w, plain, turned in ((0, wk, q_s, qt_s), (768, wv, g_s, gt_s)):
            x_h = whole(at + h * width, width)
            w_h = w[:, cols]
            straight = dot(x_h, w_h, ((1,), (1,))).astype(bf16)
            across = dot(w_h, x_h, ((1,), (1,))).astype(bf16)
            for i in range(GROUP):
                plain[i, rows, 0:512] = straight[i * toks : (i + 1) * toks, :]
                lanes = slice((i % 2 * heads + h) * toks, (i % 2 * heads + h + 1) * toks)
                turned[i // 2, 0:512, lanes] = across[:, i * toks : (i + 1) * toks]
        for i in range(GROUP):
            qr_h = qs[i, :, 512 + h * 64 : 512 + (h + 1) * 64]
            q_s[i, rows, 512:576] = qr_h
            lanes = slice((i % 2 * heads + h) * toks, (i % 2 * heads + h + 1) * toks)
            qt_s[i // 2, 512:576, lanes] = qr_h.T
            extra = qs[i, :, 1280:1408].astype(f32)
            for k, ref in enumerate((log_s, term_s)):
                at = (h * 2 + k) * 3
                value = extra[:, at : at + 1] + extra[:, at + 1 : at + 2] + extra[:, at + 2 : at + 3]
                ref[i, rows, :] = jnp.broadcast_to(value, (toks, 128))

    own_key = lax.broadcasted_iota(jnp.int32, (1, 2 * toks), 1) < toks
    key_c = jnp.where(own_key, my_c, 1 - my_c)

    def plane(p, _):
        @pl.when((p == 0) | (info[jnp.maximum(p - 1, 0)] == 1))
        def _():
            for i, ref in enumerate((k0, k1, k2, k3)):

                @pl.when(p == i)
                def _(ref=ref):
                    kcur[0:toks, :] = ref[...]

            kcur[toks : 2 * toks, :] = kother[p]

            def chunks(j, _):
                lows, slopes_low = [], []
                for half in range(2):
                    i = 2 * j + half
                    ahead = ((i - my_x) * 2 + my_c - key_c) * toks
                    limit = ahead + jnp.where(p == 0, 0, 1 << 20)
                    scores = dot(q_s[i], kcur[...], ((1,), (1,)))
                    slopes = dot(g_s[i], kcur[:, 0:512], ((1,), (1,)))
                    logs = jnp.concatenate([log_s[i]] * 2, axis=1)
                    terms = jnp.concatenate([term_s[i]] * 2, axis=1)
                    weights = jnp.exp(factor * scores - logs)
                    weights = jnp.where(gap_s[...] <= limit, weights, 0.0)
                    dscores = (weights * (slopes - terms)).astype(bf16)
                    acc[i] += dot(dscores, kcur[...], ((1,), (0,)))
                    lows.append(weights.astype(bf16))
                    slopes_low.append(dscores)
                ds_acc[p] += dot(qt_s[j], jnp.concatenate(slopes_low, axis=0), ((1,), (0,)))
                w_acc[p] += dot(gt_s[j], jnp.concatenate(lows, axis=0), ((1,), (0,)))
                return 0

            lax.fori_loop(jnp.where((p == 0) & (my_x >= 2), 1, 0), GROUP // 2, chunks, 0)

        return 0

    lax.fori_loop(0, GROUP, plane, 0)
    for h in range(heads):
        rows = slice(h * toks, (h + 1) * toks)
        cols = slice(h * width, (h + 1) * width)
        mixed = acc[:, rows, 0:512].reshape(GROUP * toks, 512)
        high = mixed.astype(bf16)
        low = (mixed - high.astype(f32)).astype(bf16)
        w_h = wk[:, cols]
        main = factor * (dot(high, w_h, ((1,), (0,))) + dot(low, w_h, ((1,), (0,))))
        x_h = whole(h * width, width)
        wt_acc[cols, :] = dot(x_h, high, ((0,), (0,))) + dot(x_h, low, ((0,), (0,)))
        for i in range(GROUP):
            back_s[i, rows, :] = main[i * toks : (i + 1) * toks, :]
    for i in range(GROUP):
        for h in range(2):
            pair = [acc[i, (2 * h + k) * toks : (2 * h + k + 1) * toks, 512:576] for k in range(2)]
            rows = slice((heads + h) * toks, (heads + h + 1) * toks)
            back_s[i, rows, :] = factor * jnp.concatenate(pair, axis=1)
    for p in range(GROUP):
        for rows in (slice(0, 512), slice(512, 576)):
            both = factor * ds_acc[p, rows, :]
            if rows.start == 0:
                both = both + w_acc[p]
            mine[p, rows, :] = both[:, 0:toks]
            theirs[p, rows, :] = both[:, toks : 2 * toks]
    wt_acc[...] = factor * wt_acc[...].T
    upper = lax.broadcasted_iota(jnp.int32, (8, 512), 0) < 4
    for x in range(4):
        for b in range(4):
            for pair in range(2):
                one, two = (
                    wt_acc[(((8 * pair + 4 * g + b + 15) % 16) * 4 + x) * 8 :][:8] for g in range(2)
                )
                even = jnp.where(upper, one, pltpu.roll(two, 4, 0))
                odd = jnp.where(upper, pltpu.roll(one, 4, 0), two)
                at = 768 + (b * 2 + pair) * 32
                for first, tile in enumerate((even, odd)):
                    for k in range(4):
                        lanes = slice(k * 128, (k + 1) * 128)
                        rows = slice(at + first * 256 + k * 8, at + first * 256 + k * 8 + 8)
                        back_s[x, rows, :] = tile[:, lanes]
    back[...] = back_s[...].astype(bf16)


def attend(info, qs, ks, kother, wk, wv):
    toks = 128
    out = jax.ShapeDtypeStruct
    vmem = pl.BlockSpec(memory_space=pltpu.VMEM)
    return pl.pallas_call(
        attend_kernel,
        in_specs=[pl.BlockSpec(memory_space=pltpu.SMEM)] + [vmem] * 8,
        out_specs=[vmem] * 3,
        out_shape=[
            out((4, 1280, 128), bf16),
            out((GROUP, 576, toks), f32),
            out((GROUP, 576, toks), f32),
        ],
        scratch_shapes=[
            pltpu.VMEM((2 * toks, 640), bf16),
            pltpu.VMEM((GROUP, 512, 640), bf16),
            pltpu.VMEM((GROUP // 2, 576, 1024), bf16),
            pltpu.VMEM((GROUP, 512, 512), bf16),
            pltpu.VMEM((GROUP // 2, 512, 1024), bf16),
            pltpu.VMEM((GROUP, 512, 128), f32),
            pltpu.VMEM((GROUP, 512, 128), f32),
            pltpu.VMEM((512, 2 * toks), jnp.int32),
            pltpu.VMEM((GROUP, 512, 640), f32),
            pltpu.VMEM((GROUP, 576, 2 * toks), f32),
            pltpu.VMEM((GROUP, 512, 2 * toks), f32),
            pltpu.VMEM((512, 512), f32),
            pltpu.VMEM((4, 1280, 128), f32),
        ],
        compiler_params=pltpu.CompilerParams(vmem_limit_bytes=52 << 20),
        name="attend",
    )(info, qs, *ks, kother, wk, wv)


def local(body, shapes, *args, scalars=0, scratch=(), aliases=None):
    vmem = pl.BlockSpec(memory_space=pltpu.VMEM)
    smem = pl.BlockSpec(memory_space=pltpu.SMEM)
    return pl.pallas_call(
        body,
        in_specs=[smem] * scalars + [vmem] * (len(args) - scalars),
        out_specs=[vmem] * len(shapes),
        out_shape=[jax.ShapeDtypeStruct(s, t) for s, t in shapes],
        scratch_shapes=list(scratch),
        input_output_aliases=aliases or {},
        compiler_params=pltpu.CompilerParams(vmem_limit_bytes=4 << 20),
    )(*args)


def stack_kernel(k0, k1, k2, k3, out):
    for i, k in enumerate((k0, k1, k2, k3)):
        out[i] = k[...]


def pair_kernel(mine, theirs, z0, z1, z2, z3):
    for p, out in enumerate((z0, z1, z2, z3)):
        out[...] = (mine[p] + theirs[p]).astype(out.dtype)


def added(parts):
    return (parts[0] + parts[1]) + (parts[2] + parts[3])


def back_kernel(back, main, rotary, near):
    def rows(start, count):
        return added([back[i, start : start + count, :].astype(f32) for i in range(4)])

    for h in range(4):
        main[:, h * 128 : (h + 1) * 128] = rows(h * 128, 128)
    for h in range(2):
        rotary[:, h * 128 : (h + 1) * 128] = rows(512 + h * 128, 128)
    for b in range(4):
        for c in range(2):
            near[2 * b + c] = rows(768 + c * 256 + b * 64, 64)


def couple_kernel(mine, theirs, total):
    total[...] = (mine[...].astype(f32) + theirs[...].astype(f32)).astype(bf16)


def key_kernel(z0, z1, z2, z3, key):
    key[...] = added([z[...].astype(f32) for z in (z0, z1, z2, z3)]).astype(bf16)


def far_kernel(near, far):
    total = added([near[i] + near[i + 4] for i in range(4)])
    for pair in range(2):
        for k in range(4):
            tile = total[pair * 32 + k * 8 :][:8]
            far[2 * pair, k * 8 : k * 8 + 8, :] = tile
            far[2 * pair + 1, k * 8 : k * 8 + 8, :] = pltpu.roll(tile, 4, 0)


def last_kernel(keys, other_keys, far, lat, rot, weight):
    total = keys[...].astype(f32) + other_keys[...].astype(f32)
    lat[...] = total[0:512, :].T
    rot[...] = total[512:576, :]
    for k in range(4):
        part = added([far[i, k * 8 : k * 8 + 4, :] for i in range(4)])
        weight[:, k * 128 : (k + 1) * 128] = part


def swap(block, axis, bit):
    pairs = [(i, i ^ bit) for i in range(lax.axis_size(axis))]
    return lax.ppermute(block, axis, pairs)


def exchange(tiles, axis, groups=None):
    return lax.all_to_all(tiles, axis, 0, 0, tiled=True, axis_index_groups=groups)


def per_device(
    query_main,
    query_rotary,
    latent,
    key_rotary,
    key_weight,
    value_weight,
    head_output,
    output_grad,
    row_logsum,
):
    my_z, my_x, my_c = (lax.axis_index(a) for a in SP)
    planes = lax.axis_size(Z)
    seq = (my_z + 1) // GROUP
    flags = [
        ((my_z >= s) & ((my_z - s + 1) // GROUP == seq)).astype(jnp.int32) for s in range(1, GROUP)
    ]
    info = jnp.stack([*flags, my_x, my_c]).astype(jnp.int32)
    qpack, kpack = pack(
        query_main, query_rotary, output_grad, head_output, row_logsum, latent, key_rotary.T
    )
    ks = [kpack]
    for s in range(1, GROUP):
        ks.append(onward(kpack, s))
    qs = exchange(qpack, X)
    (stacked,) = local(stack_kernel, [((4, *kpack.shape), bf16)], *ks)
    kother = shift(stacked, C, 1)
    back, mine, theirs = attend(info, qs, ks, kother, key_weight, value_weight)
    back = exchange(back, X)
    theirs = shift(theirs, C, 1)
    shapes = [((576, 128), f32)] + [((576, 128), bf16)] * 3
    planes = local(pair_kernel, shapes, mine, theirs)
    planes = list(planes)
    for s in range(1, 4):
        planes[s] = onward(planes[s], -s)
    toks = key_rotary.shape[0]
    shapes = [((toks, 512), f32), ((toks, 256), f32), ((8, 64, 128), f32)]
    main, rotary, weight = local(back_kernel, shapes, back)
    near = [[(4 * g + b - 1) % 16 for b in range(4)] for g in range(4)]
    pairs = [[2 * z + c for z in zs for c in range(2)] for zs in near]
    weight = exchange(weight, (Z, C), pairs)
    (key,) = local(key_kernel, [((576, 128), bf16)], *planes)
    beside = swap(key, Y, 1)
    (key,) = local(couple_kernel, [((576, 128), bf16)], key, beside)
    across = swap(key, Y, 2)
    (weight,) = local(far_kernel, [((4, 32, 128), f32)], weight)
    weight = exchange(weight, Z, [list(z) for z in zip(*near)])
    shapes = [((toks, 512), f32), ((64, toks), f32), ((4, 512), f32)]
    lat, rot, weight = local(last_kernel, shapes, key, across, weight)
    return main, rotary, lat, rot.T, weight


def solution(mesh):
    finer = Mesh(mesh.devices.reshape(16, 4, 2, mesh.shape["tp"]), (Z, X, C, Y))
    return jax.shard_map(
        per_device,
        mesh=finer,
        in_specs=(
            P(SP, "tp"),
            P(SP, "tp"),
            P(SP, None),
            P(SP, None),
            P(None, "tp"),
            P(None, "tp"),
            P(SP, "tp"),
            P(SP, "tp"),
            P("tp", SP),
        ),
        out_specs=(P(SP, "tp"), P(SP, "tp"), P(SP, None), P(SP, None), P(SP, "tp")),
        check_vma=False,
    )
```

```python
import jax
import jax.numpy as jnp
from jax import lax
from jax.experimental import pallas as pl
from jax.experimental.pallas import tpu as pltpu
from jax.sharding import Mesh
from jax.sharding import PartitionSpec as P


Z, X, C, Y = "sp_0", "sp_1", "sp_2", "tp"
SP = (Z, X, C)
GROUP = 4
bf16 = jnp.bfloat16
f32 = jnp.float32


def shift(block, axis, by):
    peers = lax.axis_size(axis)
    return lax.ppermute(block, axis, [(i, (i + by) % peers) for i in range(peers)])


def onward(block, by):
    planes = lax.axis_size(Z)
    ends = [(i, i + by) for i in range(planes)]
    pairs = [(i, j) for i, j in ends if 0 <= j < planes and (i + 1) // GROUP == (j + 1) // GROUP]
    return lax.ppermute(block, Z, pairs)


def dot(a, b, dims):
    return lax.dot_general(a, b, (dims, ((), ())), preferred_element_type=f32)


def pack_kernel(qm, qr, og, ho, logs, lat, rot, qpack, kpack):
    heads, toks = logs.shape
    width = qm.shape[1] // heads
    lane = lax.broadcasted_iota(jnp.int32, (toks, 128), 1)
    extra = jnp.zeros((toks, 128), f32)
    logs_t = logs[...].T
    for h in range(heads):
        cols = slice(h * width, (h + 1) * width)
        term = jnp.sum(ho[:, cols].astype(f32) * og[:, cols].astype(f32), axis=1, keepdims=True)
        for k, value in enumerate((logs_t[:, h : h + 1], term)):
            for part in range(3):
                piece = value.astype(bf16).astype(f32)
                value = value - piece
                extra = jnp.where(lane == (h * 2 + k) * 3 + part, piece, extra)
    for i in range(qpack.shape[0]):
        qpack[i, :, 0:512] = qm[...]
        qpack[i, :, 512:768] = qr[...]
        qpack[i, :, 768:1280] = og[...]
        qpack[i, :, 1280:1408] = extra.astype(bf16)
    kpack[:, 0:512] = lat[...]
    kpack[:, 512:576] = rot[...].T
    kpack[:, 576:640] = jnp.zeros((toks, 64), bf16)


def pack(*args):
    toks = args[0].shape[0]
    return pl.pallas_call(
        pack_kernel,
        out_shape=(
            jax.ShapeDtypeStruct((4, toks, 1408), bf16),
            jax.ShapeDtypeStruct((toks, 640), bf16),
        ),
        name="pack",
    )(*args)


def attend_kernel(
    info, qs, k0, k1, k2, k3, kother, wk, wv,
    back, mine, theirs,
    kcur, q_s, qt_s, g_s, gt_s, log_s, term_s, gap_s, acc, ds_acc, w_acc, wt_acc, back_s,
):
    heads, toks, width = 4, 128, 128
    factor = 192.0**-0.5
    my_x = info[3]
    my_c = info[4]

    def whole(start, count):
        return qs[:, :, start : start + count].reshape(GROUP * toks, count)

    acc[...] = jnp.zeros_like(acc)
    ds_acc[...] = jnp.zeros_like(ds_acc)
    w_acc[...] = jnp.zeros_like(w_acc)
    shape = (heads * toks, 2 * toks)
    gap_s[...] = (
        lax.broadcasted_iota(jnp.int32, shape, 1) % toks
        - lax.broadcasted_iota(jnp.int32, shape, 0) % toks
    )
    for j in range(GROUP // 2):
        q_s[j, :, 576:640] = jnp.zeros((2 * heads * toks, 64), bf16)
    for h in range(heads):
        rows = slice(h * toks, (h + 1) * toks)
        cols = slice(h * width, (h + 1) * width)
        for at, w, plain, turned in ((0, wk, q_s, qt_s), (768, wv, g_s, gt_s)):
            x_h = whole(at + h * width, width)
            w_h = w[:, cols]
            straight = dot(x_h, w_h, ((1,), (1,))).astype(bf16)
            across = dot(w_h, x_h, ((1,), (1,))).astype(bf16)
            for i in range(GROUP):
                lanes = slice((i % 2 * heads + h) * toks, (i % 2 * heads + h + 1) * toks)
                plain[i // 2, lanes, 0:512] = straight[i * toks : (i + 1) * toks, :]
                turned[i // 2, 0:512, lanes] = across[:, i * toks : (i + 1) * toks]
        for i in range(GROUP):
            qr_h = qs[i, :, 512 + h * 64 : 512 + (h + 1) * 64]
            lanes = slice((i % 2 * heads + h) * toks, (i % 2 * heads + h + 1) * toks)
            q_s[i // 2, lanes, 512:576] = qr_h
            qt_s[i // 2, 512:576, lanes] = qr_h.T
            extra = qs[i, :, 1280:1408].astype(f32)
            for k, ref in enumerate((log_s, term_s)):
                at = (h * 2 + k) * 3
                value = extra[:, at : at + 1] + extra[:, at + 1 : at + 2] + extra[:, at + 2 : at + 3]
                ref[i, rows, :] = jnp.broadcast_to(value, (toks, 128))

    own_key = lax.broadcasted_iota(jnp.int32, (1, 2 * toks), 1) < toks
    key_c = jnp.where(own_key, my_c, 1 - my_c)

    def plane(p, _):
        @pl.when((p == 0) | (info[jnp.maximum(p - 1, 0)] == 1))
        def _():
            for i, ref in enumerate((k0, k1, k2, k3)):

                @pl.when(p == i)
                def _(ref=ref):
                    kcur[0:toks, :] = ref[...]

            kcur[toks : 2 * toks, :] = kother[p]

            def chunks(j, _):
                lows, slopes_low = [], []
                both_scores = dot(q_s[j], kcur[...], ((1,), (1,)))
                both_slopes = dot(g_s[j], kcur[:, 0:512], ((1,), (1,)))
                for half in range(2):
                    i = 2 * j + half
                    part = slice(half * heads * toks, (half + 1) * heads * toks)
                    ahead = ((i - my_x) * 2 + my_c - key_c) * toks
                    limit = ahead + jnp.where(p == 0, 0, 1 << 20)
                    scores = both_scores[part, :]
                    slopes = both_slopes[part, :]
                    logs = jnp.concatenate([log_s[i]] * 2, axis=1)
                    terms = jnp.concatenate([term_s[i]] * 2, axis=1)
                    weights = jnp.exp(factor * scores - logs)
                    weights = jnp.where(gap_s[...] <= limit, weights, 0.0)
                    dscores = (weights * (slopes - terms)).astype(bf16)
                    acc[i] += dot(dscores, kcur[...], ((1,), (0,)))
                    lows.append(weights.astype(bf16))
                    slopes_low.append(dscores)
                ds_acc[p] += dot(qt_s[j], jnp.concatenate(slopes_low, axis=0), ((1,), (0,)))
                w_acc[p] += dot(gt_s[j], jnp.concatenate(lows, axis=0), ((1,), (0,)))
                return 0

            lax.fori_loop(jnp.where((p == 0) & (my_x >= 2), 1, 0), GROUP // 2, chunks, 0)

        return 0

    lax.fori_loop(0, GROUP, plane, 0)
    for h in range(heads):
        rows = slice(h * toks, (h + 1) * toks)
        cols = slice(h * width, (h + 1) * width)
        mixed = acc[:, rows, 0:512].reshape(GROUP * toks, 512)
        high = mixed.astype(bf16)
        low = (mixed - high.astype(f32)).astype(bf16)
        w_h = wk[:, cols]
        main = factor * (dot(high, w_h, ((1,), (0,))) + dot(low, w_h, ((1,), (0,))))
        x_h = whole(h * width, width)
        wt_acc[cols, :] = dot(x_h, high, ((0,), (0,))) + dot(x_h, low, ((0,), (0,)))
        for i in range(GROUP):
            back_s[i, rows, :] = main[i * toks : (i + 1) * toks, :]
    for i in range(GROUP):
        for h in range(2):
            pair = [acc[i, (2 * h + k) * toks : (2 * h + k + 1) * toks, 512:576] for k in range(2)]
            rows = slice((heads + h) * toks, (heads + h + 1) * toks)
            back_s[i, rows, :] = factor * jnp.concatenate(pair, axis=1)
    for p in range(GROUP):
        for rows in (slice(0, 512), slice(512, 576)):
            both = factor * ds_acc[p, rows, :]
            if rows.start == 0:
                both = both + w_acc[p]
            mine[p, rows, :] = both[:, 0:toks]
            theirs[p, rows, :] = both[:, toks : 2 * toks]
    wt_acc[...] = factor * wt_acc[...].T
    upper = lax.broadcasted_iota(jnp.int32, (8, 512), 0) < 4
    for x in range(4):
        for b in range(4):
            for pair in range(2):
                one, two = (
                    wt_acc[(((8 * pair + 4 * g + b + 15) % 16) * 4 + x) * 8 :][:8] for g in range(2)
                )
                even = jnp.where(upper, one, pltpu.roll(two, 4, 0))
                odd = jnp.where(upper, pltpu.roll(one, 4, 0), two)
                at = 768 + (b * 2 + pair) * 32
                for first, tile in enumerate((even, odd)):
                    for k in range(4):
                        lanes = slice(k * 128, (k + 1) * 128)
                        rows = slice(at + first * 256 + k * 8, at + first * 256 + k * 8 + 8)
                        back_s[x, rows, :] = tile[:, lanes]
    back[...] = back_s[...].astype(bf16)


def attend(info, qs, ks, kother, wk, wv):
    toks = 128
    out = jax.ShapeDtypeStruct
    vmem = pl.BlockSpec(memory_space=pltpu.VMEM)
    return pl.pallas_call(
        attend_kernel,
        in_specs=[pl.BlockSpec(memory_space=pltpu.SMEM)] + [vmem] * 8,
        out_specs=[vmem] * 3,
        out_shape=[
            out((4, 1280, 128), bf16),
            out((GROUP, 576, toks), f32),
            out((GROUP, 576, toks), f32),
        ],
        scratch_shapes=[
            pltpu.VMEM((2 * toks, 640), bf16),
            pltpu.VMEM((GROUP // 2, 1024, 640), bf16),
            pltpu.VMEM((GROUP // 2, 576, 1024), bf16),
            pltpu.VMEM((GROUP // 2, 1024, 512), bf16),
            pltpu.VMEM((GROUP // 2, 512, 1024), bf16),
            pltpu.VMEM((GROUP, 512, 128), f32),
            pltpu.VMEM((GROUP, 512, 128), f32),
            pltpu.VMEM((512, 2 * toks), jnp.int32),
            pltpu.VMEM((GROUP, 512, 640), f32),
            pltpu.VMEM((GROUP, 576, 2 * toks), f32),
            pltpu.VMEM((GROUP, 512, 2 * toks), f32),
            pltpu.VMEM((512, 512), f32),
            pltpu.VMEM((4, 1280, 128), f32),
        ],
        compiler_params=pltpu.CompilerParams(vmem_limit_bytes=52 << 20),
        name="attend",
    )(info, qs, *ks, kother, wk, wv)


def local(body, shapes, *args, scalars=0, scratch=(), aliases=None):
    vmem = pl.BlockSpec(memory_space=pltpu.VMEM)
    smem = pl.BlockSpec(memory_space=pltpu.SMEM)
    return pl.pallas_call(
        body,
        in_specs=[smem] * scalars + [vmem] * (len(args) - scalars),
        out_specs=[vmem] * len(shapes),
        out_shape=[jax.ShapeDtypeStruct(s, t) for s, t in shapes],
        scratch_shapes=list(scratch),
        input_output_aliases=aliases or {},
        compiler_params=pltpu.CompilerParams(vmem_limit_bytes=4 << 20),
    )(*args)


def stack_kernel(k0, k1, k2, k3, out):
    for i, k in enumerate((k0, k1, k2, k3)):
        out[i] = k[...]


def pair_kernel(mine, theirs, z0, z1, z2, z3):
    for p, out in enumerate((z0, z1, z2, z3)):
        out[...] = (mine[p] + theirs[p]).astype(out.dtype)


def added(parts):
    return (parts[0] + parts[1]) + (parts[2] + parts[3])


def back_kernel(back, main, rotary, near):
    def rows(start, count):
        return added([back[i, start : start + count, :].astype(f32) for i in range(4)])

    for h in range(4):
        main[:, h * 128 : (h + 1) * 128] = rows(h * 128, 128)
    for h in range(2):
        rotary[:, h * 128 : (h + 1) * 128] = rows(512 + h * 128, 128)
    for b in range(4):
        for c in range(2):
            near[2 * b + c] = rows(768 + c * 256 + b * 64, 64)


def couple_kernel(mine, theirs, total):
    total[...] = (mine[...].astype(f32) + theirs[...].astype(f32)).astype(bf16)


def key_kernel(z0, z1, z2, z3, key):
    key[...] = added([z[...].astype(f32) for z in (z0, z1, z2, z3)]).astype(bf16)


def far_kernel(near, far):
    total = added([near[i] + near[i + 4] for i in range(4)])
    for pair in range(2):
        for k in range(4):
            tile = total[pair * 32 + k * 8 :][:8]
            far[2 * pair, k * 8 : k * 8 + 8, :] = tile
            far[2 * pair + 1, k * 8 : k * 8 + 8, :] = pltpu.roll(tile, 4, 0)


def last_kernel(keys, other_keys, far, lat, rot, weight):
    total = keys[...].astype(f32) + other_keys[...].astype(f32)
    lat[...] = total[0:512, :].T
    rot[...] = total[512:576, :]
    for k in range(4):
        part = added([far[i, k * 8 : k * 8 + 4, :] for i in range(4)])
        weight[:, k * 128 : (k + 1) * 128] = part


def swap(block, axis, bit):
    pairs = [(i, i ^ bit) for i in range(lax.axis_size(axis))]
    return lax.ppermute(block, axis, pairs)


def exchange(tiles, axis, groups=None):
    return lax.all_to_all(tiles, axis, 0, 0, tiled=True, axis_index_groups=groups)


def per_device(
    query_main,
    query_rotary,
    latent,
    key_rotary,
    key_weight,
    value_weight,
    head_output,
    output_grad,
    row_logsum,
):
    my_z, my_x, my_c = (lax.axis_index(a) for a in SP)
    planes = lax.axis_size(Z)
    seq = (my_z + 1) // GROUP
    flags = [
        ((my_z >= s) & ((my_z - s + 1) // GROUP == seq)).astype(jnp.int32) for s in range(1, GROUP)
    ]
    info = jnp.stack([*flags, my_x, my_c]).astype(jnp.int32)
    qpack, kpack = pack(
        query_main, query_rotary, output_grad, head_output, row_logsum, latent, key_rotary.T
    )
    ks = [kpack]
    for s in range(1, GROUP):
        ks.append(onward(kpack, s))
    qs = exchange(qpack, X)
    (stacked,) = local(stack_kernel, [((4, *kpack.shape), bf16)], *ks)
    kother = shift(stacked, C, 1)
    back, mine, theirs = attend(info, qs, ks, kother, key_weight, value_weight)
    back = exchange(back, X)
    theirs = shift(theirs, C, 1)
    shapes = [((576, 128), f32)] + [((576, 128), bf16)] * 3
    planes = local(pair_kernel, shapes, mine, theirs)
    planes = list(planes)
    for s in range(1, 4):
        planes[s] = onward(planes[s], -s)
    toks = key_rotary.shape[0]
    shapes = [((toks, 512), f32), ((toks, 256), f32), ((8, 64, 128), f32)]
    main, rotary, weight = local(back_kernel, shapes, back)
    near = [[(4 * g + b - 1) % 16 for b in range(4)] for g in range(4)]
    pairs = [[2 * z + c for z in zs for c in range(2)] for zs in near]
    weight = exchange(weight, (Z, C), pairs)
    (key,) = local(key_kernel, [((576, 128), bf16)], *planes)
    beside = swap(key, Y, 1)
    (key,) = local(couple_kernel, [((576, 128), bf16)], key, beside)
    across = swap(key, Y, 2)
    (weight,) = local(far_kernel, [((4, 32, 128), f32)], weight)
    weight = exchange(weight, Z, [list(z) for z in zip(*near)])
    shapes = [((toks, 512), f32), ((64, toks), f32), ((4, 512), f32)]
    lat, rot, weight = local(last_kernel, shapes, key, across, weight)
    return main, rotary, lat, rot.T, weight


def solution(mesh):
    finer = Mesh(mesh.devices.reshape(16, 4, 2, mesh.shape["tp"]), (Z, X, C, Y))
    return jax.shard_map(
        per_device,
        mesh=finer,
        in_specs=(
            P(SP, "tp"),
            P(SP, "tp"),
            P(SP, None),
            P(SP, None),
            P(None, "tp"),
            P(None, "tp"),
            P(SP, "tp"),
            P(SP, "tp"),
            P("tp", SP),
        ),
        out_specs=(P(SP, "tp"), P(SP, "tp"), P(SP, None), P(SP, None), P(SP, "tp")),
        check_vma=False,
    )
```
